32 devices in a mesh: tp: 32 (over z, y, x, core).
Axes of the slice: x: 2, y: 2, z: 4, core: 2. Of those that a mesh axis runs over, the one named last changes fastest.
Arguments:
- tokens: bfloat16 [32, 8, 4096], P('tp'), may hold values from -6 to 6
- block_norm_gain: float32 [2, 4096], replicated, may hold values from 0.1 to 1.9
- receptance_weight: bfloat16 [2, 32, 4096, 64], P(None, 'tp'), may hold values from -0.09375 to 0.09375
- key_weight: bfloat16 [2, 32, 4096, 64], P(None, 'tp'), may hold values from -0.09375 to 0.09375
- value_weight: bfloat16 [2, 32, 4096, 64], P(None, 'tp'), may hold values from -0.09375 to 0.09375
- decay_weight: bfloat16 [2, 32, 4096, 64], P(None, 'tp'), may hold values from -0.09375 to 0.09375
- learning_rate_weight: bfloat16 [2, 32, 4096, 64], P(None, 'tp'), may hold values from -0.09375 to 0.09375
- gate_weight: bfloat16 [2, 32, 4096, 64], P(None, 'tp'), may hold values from -0.09375 to 0.09375
- decay_bias_fixed: float32 [2, 2048], replicated, may hold values from -5 to 2
- self_token_weight: float32 [2, 2048], replicated, may hold values from -1.5 to 1.5
- readout_norm_gain: float32 [2, 2048], replicated, may hold values from 0.1 to 1.9
- output_weight: bfloat16 [2, 32, 64, 4096], P(None, 'tp'), may hold values from -0.125 to 0.125
- state: float32 [2, 32, 256, 4096], P(None, 'tp'), may hold values from -3 to 3
Outputs:
- mixed: bfloat16 [32, 8, 4096], P('tp')
- new_state: float32 [2, 32, 256, 4096], P(None, 'tp')
The draws below stay inside these ranges and needn't reach their ends.
All inputs are finite; a program needn't handle non-finite values.
Results may differ from the reference program's by a relative error of at most 0.018.
Values may be sent and summed in bfloat16 or wider, within the bound.
No kernel may reach another device: no remote copies, remote signals or barrier semaphores. Data moves between devices by JAX's collectives and lax.ppermute only.
A program may use at most 128 MiB of HBM per device.

```python
import jax
import jax.numpy as jnp
from jax import lax

D = 4096
MIXER_WIDTH = 2048
HEAD_CHANNELS = 64
WINDOW_LAYERS = 2
SEQS = 256
MIXER_HEADS = 32
ROW_BLOCKS = 1
N_TP = 32


def shard_levels(own_key, shape, split, smallest, largest):
    gain = 1.0
    for axis_at, blocks in split:
        steps = jax.random.uniform(jax.random.fold_in(jax.random.fold_in(own_key, 6), axis_at), (blocks,), jnp.float32, smallest / len(split), largest / len(split))
        gain = gain * jnp.repeat(jnp.exp(steps), shape[axis_at] // blocks).reshape((-1,) + (1,) * (len(shape) - 1 - axis_at))
    return gain


def scatter_about(own_key, shape, width, most, pieces=(), dtype=jnp.bfloat16):
    loudness = shard_levels(own_key, shape, pieces, -0.22, 0.18) if pieces else 1.0
    entries = jax.random.normal(own_key, shape, jnp.float32) * width * loudness
    return jnp.minimum(jnp.maximum(entries, -most), most).astype(dtype)


def setup_inputs(seed: int = 0) -> dict:
    streams_of = jax.random.split(jax.random.key(seed), 14)
    tokens = scatter_about(streams_of[0], (N_TP, SEQS // MIXER_HEADS, D // ROW_BLOCKS), 1.0, 6.0, ((0, 32),))
    block_norm_gain = jnp.clip(1.0 + 0.18 * jax.random.normal(streams_of[1], (WINDOW_LAYERS, D), jnp.float32), 0.1, 1.9)
    receptance_weight = scatter_about(streams_of[2], (WINDOW_LAYERS, N_TP, D // ROW_BLOCKS, HEAD_CHANNELS), D ** -0.5, 0.09375, ((1, 32),))
    key_weight = scatter_about(streams_of[3], (WINDOW_LAYERS, N_TP, D // ROW_BLOCKS, HEAD_CHANNELS), D ** -0.5, 0.09375, ((1, 32),))
    value_weight = scatter_about(streams_of[4], (WINDOW_LAYERS, N_TP, D // ROW_BLOCKS, HEAD_CHANNELS), D ** -0.5, 0.09375, ((1, 32),))
    decay_weight = scatter_about(streams_of[5], (WINDOW_LAYERS, N_TP, D // ROW_BLOCKS, HEAD_CHANNELS), D ** -0.5, 0.09375, ((1, 32),))
    learning_rate_weight = scatter_about(streams_of[6], (WINDOW_LAYERS, N_TP, D // ROW_BLOCKS, HEAD_CHANNELS), D ** -0.5, 0.09375, ((1, 32),))
    gate_weight = scatter_about(streams_of[7], (WINDOW_LAYERS, N_TP, D // ROW_BLOCKS, HEAD_CHANNELS), D ** -0.5, 0.09375, ((1, 32),))
    decay_bias_fixed = jnp.clip(jax.random.uniform(streams_of[8], (WINDOW_LAYERS, MIXER_WIDTH), jnp.float32, -5.0, 2.0), -5.0, 2.0)
    self_token_weight = scatter_about(streams_of[9], (WINDOW_LAYERS, MIXER_WIDTH), 0.3, 1.5, (), jnp.float32)
    readout_norm_gain = jnp.clip(1.0 + 0.18 * jax.random.normal(streams_of[10], (WINDOW_LAYERS, MIXER_WIDTH), jnp.float32), 0.1, 1.9)
    output_weight = scatter_about(streams_of[11], (WINDOW_LAYERS, N_TP, HEAD_CHANNELS, D // ROW_BLOCKS), MIXER_WIDTH ** -0.5, 0.125, ((1, 32),))
    state = scatter_about(streams_of[12], (WINDOW_LAYERS, N_TP, SEQS // ROW_BLOCKS, HEAD_CHANNELS * HEAD_CHANNELS), 0.5, 3.0, ((1, 32),), jnp.float32)
    return {"tokens": tokens, "block_norm_gain": block_norm_gain, "receptance_weight": receptance_weight, "key_weight": key_weight, "value_weight": value_weight, "decay_weight": decay_weight, "learning_rate_weight": learning_rate_weight, "gate_weight": gate_weight, "decay_bias_fixed": decay_bias_fixed, "self_token_weight": self_token_weight, "readout_norm_gain": readout_norm_gain, "output_weight": output_weight, "state": state}


RMS_EPS = 1e-06
GROUP_EPS = 0.00064

def recurrent_update(layer_state, receptance_vector, key_vector, value_vector, decay_logits, learning_rate_logits, gate_logits, decay_constant, self_term_scale, head_gain_slice):
    highest = lax.Precision.HIGHEST
    shrink = jnp.exp(-jnp.exp(-jax.nn.softplus(-(decay_constant + decay_logits)) - 0.5))
    rate = jax.nn.sigmoid(learning_rate_logits)
    normed = key_vector * lax.rsqrt(lax.optimization_barrier(jnp.sum(key_vector * key_vector, -1, keepdims=True)) + 1.0)
    removed = jnp.einsum('...ij,...j->...i', layer_state, normed, precision=highest)
    layer_state = layer_state * shrink[..., None, :] - removed[..., :, None] * (normed * rate)[..., None, :] + value_vector[..., :, None] * (key_vector * rate)[..., None, :]
    readout = jnp.einsum('...ij,...j->...i', layer_state, receptance_vector, precision=highest)
    center = lax.optimization_barrier(jnp.mean(readout, -1, keepdims=True))
    spread = lax.optimization_barrier(jnp.mean(jnp.square(readout - center), -1, keepdims=True))
    normed_output = (readout - center) * lax.rsqrt(spread + GROUP_EPS) * head_gain_slice
    self_term = lax.optimization_barrier(jnp.sum(receptance_vector * key_vector * self_term_scale, -1, keepdims=True)) * value_vector
    return (((normed_output + self_term) * jax.nn.sigmoid(gate_logits)).astype(jnp.bfloat16), layer_state)

def reference(tokens, block_norm_gain, receptance_weight, key_weight, value_weight, decay_weight, learning_rate_weight, gate_weight, decay_bias_fixed, self_token_weight, readout_norm_gain, output_weight, state):
    seq_tile = SEQS // MIXER_HEADS
    col_tile = D // ROW_BLOCKS
    seq_block = SEQS // ROW_BLOCKS
    resid = tokens.reshape(MIXER_HEADS, ROW_BLOCKS, seq_tile, col_tile).transpose(0, 2, 1, 3).reshape(SEQS, D)

    def rows_full(weight):
        return weight.reshape(WINDOW_LAYERS, MIXER_HEADS, ROW_BLOCKS, col_tile, HEAD_CHANNELS).transpose(0, 2, 3, 1, 4).reshape(WINDOW_LAYERS, D, MIXER_WIDTH)
    fulls = [rows_full(weight) for weight in (receptance_weight, key_weight, value_weight, decay_weight, learning_rate_weight, gate_weight)]
    out_full = output_weight.reshape(WINDOW_LAYERS, MIXER_HEADS, ROW_BLOCKS, HEAD_CHANNELS, col_tile).transpose(0, 1, 3, 2, 4).reshape(WINDOW_LAYERS, MIXER_WIDTH, D)
    layer_states_stacked = state.reshape(WINDOW_LAYERS, MIXER_HEADS, ROW_BLOCKS, seq_block, HEAD_CHANNELS, HEAD_CHANNELS).transpose(0, 2, 3, 1, 4, 5)
    layer_states_stacked = layer_states_stacked.reshape(WINDOW_LAYERS, SEQS, MIXER_HEADS, HEAD_CHANNELS, HEAD_CHANNELS)
    updated = []
    for layer_index in range(WINDOW_LAYERS):
        wide = resid.astype(jnp.float32)
        scaled = (wide * block_norm_gain[layer_index]).astype(jnp.bfloat16)
        factor = lax.rsqrt(lax.optimization_barrier(jnp.mean(wide * wide, axis=1, keepdims=True)) + RMS_EPS)
        output_pieces = [(jnp.dot(scaled, full[layer_index], preferred_element_type=jnp.float32) * factor).reshape(SEQS, MIXER_HEADS, HEAD_CHANNELS) for full in fulls]
        head_results, layer_state = recurrent_update(layer_states_stacked[layer_index], *output_pieces, decay_bias_fixed[layer_index].reshape(MIXER_HEADS, HEAD_CHANNELS), self_token_weight[layer_index].reshape(MIXER_HEADS, HEAD_CHANNELS), readout_norm_gain[layer_index].reshape(MIXER_HEADS, HEAD_CHANNELS))
        branch = jnp.dot(head_results.reshape(SEQS, MIXER_WIDTH), out_full[layer_index], preferred_element_type=jnp.float32)
        resid = (wide + branch).astype(jnp.bfloat16)
        updated.append(layer_state)
    mixed = resid.reshape(MIXER_HEADS, seq_tile, ROW_BLOCKS, col_tile).transpose(0, 2, 1, 3).reshape(N_TP, seq_tile, col_tile)
    new_state = jnp.stack(updated).reshape(WINDOW_LAYERS, ROW_BLOCKS, seq_block, MIXER_HEADS, HEAD_CHANNELS, HEAD_CHANNELS).transpose(0, 3, 1, 2, 4, 5)
    new_state = new_state.reshape(WINDOW_LAYERS, N_TP, seq_block, HEAD_CHANNELS * HEAD_CHANNELS)
    return (mixed, new_state)
```

```python
import jax
import jax.numpy as jnp
from jax import lax
from jax.experimental import pallas as pl
from jax.experimental.pallas import tpu as pltpu
from jax.sharding import PartitionSpec as P

D = 4096


RMS_EPS = 1e-06
GROUP_EPS = 0.00064


def swapped(shard, axis, stride):
    return lax.ppermute(shard, axis, [(i, i ^ 1 << stride) for i in range(lax.axis_size(axis))])


def for_sending(shard):

    def short(part):
        return part.astype(jnp.bfloat16) if part.dtype == jnp.float32 else part

    return jax.tree.map(short, shard)


def recurrent_update(
    layer_state,
    receptance_vector,
    key_vector,
    value_vector,
    decay_logits,
    learning_rate_logits,
    gate_logits,
    decay_constant,
    self_term_scale,
    head_gain_slice,
):
    highest = lax.Precision.HIGHEST
    shrink = jnp.exp(-jnp.exp(-jax.nn.softplus(-(decay_constant + decay_logits)) - 0.5))
    rate = jax.nn.sigmoid(learning_rate_logits)
    normed = key_vector * lax.rsqrt(jnp.sum(key_vector * key_vector, -1, keepdims=True) + 1.0)
    removed = jnp.einsum("...ij,...j->...i", layer_state, normed, precision=highest)
    layer_state = (
        layer_state * shrink[..., None, :]
        - removed[..., :, None] * (normed * rate)[..., None, :]
        + value_vector[..., :, None] * (key_vector * rate)[..., None, :]
    )
    readout = jnp.einsum("...ij,...j->...i", layer_state, receptance_vector, precision=highest)
    center = jnp.mean(readout, -1, keepdims=True)
    spread = jnp.mean(jnp.square(readout - center), -1, keepdims=True)
    normed_output = (readout - center) * lax.rsqrt(spread + GROUP_EPS) * head_gain_slice
    self_term = (
        jnp.sum(receptance_vector * key_vector * self_term_scale, -1, keepdims=True) * value_vector
    )
    return (
        ((normed_output + self_term) * jax.nn.sigmoid(gate_logits)).astype(jnp.bfloat16),
        layer_state,
    )


def double_gather(piece, position, first_bit, count, mover):
    for offset in range(count):
        which_bit = first_bit + offset
        partner = mover(piece, which_bit)
        lower_self = position >> which_bit & 1 == 0
        piece = jnp.where(
            lower_self, jnp.concatenate([piece, partner], 0), jnp.concatenate([partner, piece], 0)
        )
    return piece


def halve_sum(members, position, first_bit, count, mover):
    for offset in reversed(range(count)):
        which_bit = first_bit + offset
        upper_self = position >> which_bit & 1 == 1
        sends = tuple(
            (
                jnp.where(
                    upper_self, member[: member.shape[0] // 2], member[member.shape[0] // 2 :]
                )
                for member in members
            )
        )
        keeps = tuple(
            (
                jnp.where(
                    upper_self, member[member.shape[0] // 2 :], member[: member.shape[0] // 2]
                )
                for member in members
            )
        )
        arrived = mover(sends, which_bit)
        members = tuple((kept + got for kept, got in zip(keeps, arrived)))
    return members


def on_device_blocked(
    tokens,
    block_norm_gain,
    receptance_weight,
    key_weight,
    value_weight,
    decay_weight,
    learning_rate_weight,
    gate_weight,
    decay_bias_fixed,
    self_token_weight,
    readout_norm_gain,
    output_weight,
    state,
):
    columns_dev = tokens.shape[2]
    row_blocks = D // columns_dev
    low_bits = row_blocks.bit_length() - 1
    head_count = lax.axis_size("tp") // row_blocks
    high_bits = head_count.bit_length() - 1
    position = lax.axis_index("tp")
    head_index = position // row_blocks
    row_block = position % row_blocks
    head_size = receptance_weight.shape[3]
    seq_tile = tokens.shape[1]
    move_rows = lambda payload, which_bit: swapped(payload, "tp", which_bit)
    move_proj = lambda payload, which_bit: swapped(payload, "tp", which_bit)
    move_outs = lambda payload, which_bit: jax.tree.map(
        lambda part, own: part.astype(own.dtype),
        swapped(for_sending(payload), "tp", which_bit),
        payload,
    )
    move_split = lambda payload, which_bit: jax.tree.map(
        lambda part, own: part.astype(own.dtype),
        swapped(for_sending(payload), "tp", which_bit),
        payload,
    )

    def mixer(columns, layer_index):
        gain_cols = lax.dynamic_slice_in_dim(
            block_norm_gain[layer_index], row_block * columns_dev, columns_dev
        )
        wide = columns.astype(jnp.float32)
        scaled = (wide * gain_cols).astype(jnp.bfloat16)
        squares = jnp.sum(wide * wide, axis=1)
        weights = jnp.concatenate(
            [
                receptance_weight[layer_index, 0],
                key_weight[layer_index, 0],
                value_weight[layer_index, 0],
                decay_weight[layer_index, 0],
                learning_rate_weight[layer_index, 0],
                gate_weight[layer_index, 0],
            ],
            axis=1,
        )
        partial_value = jnp.dot(scaled, weights, preferred_element_type=jnp.float32)
        summed, total_sq = halve_sum((partial_value, squares), position, 0, low_bits, move_proj)
        projected = summed * lax.rsqrt(total_sq / D + RMS_EPS)[:, None]
        output_pieces = jnp.split(projected, 6, axis=1)

        def head_columns(table):
            return lax.dynamic_slice_in_dim(table[layer_index], head_index * head_size, head_size)

        layer_state = state[layer_index, 0].reshape(-1, head_size, head_size)
        out_tile, layer_state = recurrent_update(
            layer_state,
            *output_pieces,
            head_columns(decay_bias_fixed),
            head_columns(self_token_weight),
            head_columns(readout_norm_gain)
        )
        out_all = double_gather(out_tile, position, 0, low_bits, move_outs)
        branch = jnp.dot(out_all, output_weight[layer_index, 0], preferred_element_type=jnp.float32)
        return (branch, layer_state.reshape(layer_state.shape[0], head_size * head_size))

    columns = double_gather(tokens[0], position, low_bits, high_bits, move_rows)
    first_branch, first_memory = mixer(columns, 0)
    (tile_sum,) = halve_sum((first_branch,), position, low_bits, high_bits, move_split)
    tile_one = (tokens[0].astype(jnp.float32) + tile_sum).astype(jnp.bfloat16)
    columns = double_gather(tile_one, position, low_bits, high_bits, move_rows)
    second_branch, second_memory = mixer(columns, 1)
    (tile_sum,) = halve_sum((second_branch,), position, low_bits, high_bits, move_split)
    resid_rows = lax.dynamic_slice_in_dim(columns, head_index * seq_tile, seq_tile, 0)
    mixed = (resid_rows.astype(jnp.float32) + tile_sum).astype(jnp.bfloat16)
    new_state = jnp.stack([first_memory, second_memory])[:, None]
    return (mixed[None], new_state)


CORES = 2
PLANE = 4
STATE_ROWS = 64


def moved(part, mask):
    return lax.ppermute(part, "tp", [(i, i ^ mask) for i in range(lax.axis_size("tp"))])


def slots(place_ref, rows, seq_tile):
    chips = rows // seq_tile // CORES
    levels = chips // PLANE
    for off_core in range(CORES):
        for apart in range(PLANE):
            for level in range(levels):
                chip = place_ref[0] ^ (apart + PLANE * level)
                tile = chip * CORES + (place_ref[1] ^ off_core)
                yield pl.multiple_of(tile * seq_tile, seq_tile)


def load_kernel(*refs, layers, head_size):
    count = len(refs) - 1 - layers
    weight_refs, out_refs, arrived = refs[:count], refs[count:-1], refs[-1]
    copies = [
        pltpu.make_async_copy(
            ref.at[layer, 0],
            out_refs[layer].at[at * head_size : (at + 1) * head_size, :],
            arrived.at[layer * count + at],
        )
        for layer in range(layers)
        for at, ref in enumerate(weight_refs)
    ]
    for copy in copies:
        copy.start()
    for copy in copies:
        copy.wait()


def load(weights):
    layers, _, head_size, columns = weights[0].shape
    packed = (len(weights) * head_size, columns)
    return pl.pallas_call(
        lambda *refs: load_kernel(*refs, layers=layers, head_size=head_size),
        name="load",
        in_specs=[pl.BlockSpec(memory_space=pltpu.HBM)] * len(weights),
        out_specs=[pl.BlockSpec(memory_space=pltpu.VMEM)] * layers,
        out_shape=[jax.ShapeDtypeStruct(packed, jnp.bfloat16)] * layers,
        scratch_shapes=[pltpu.SemaphoreType.DMA((layers * len(weights),))],
        compiler_params=pltpu.CompilerParams(vmem_limit_bytes=57 << 20),
    )(*weights)


def front_kernel(place_ref, *refs, piece_rows, seq_tile, head_size, layer):
    pieces = refs[: len(piece_rows)]
    (
        gain_ref,
        bias_ref,
        self_ref,
        readout_ref,
        weights_ref,
        state_ref,
        out_ref,
        vec_ref,
        scaled_ref,
        fold_ref,
        rows_ref,
        arrived,
    ) = refs[len(piece_rows) :]
    wide = 2 * head_size
    seqs, columns = rows_ref.shape
    core = place_ref[1]
    for slot, at in enumerate(slots(place_ref, seqs, seq_tile)):
        pltpu.make_async_copy(
            state_ref.at[layer, 0, pl.ds(at, seq_tile)],
            rows_ref.at[slot * seq_tile : (slot + 1) * seq_tile],
            arrived.at[slot * seq_tile // STATE_ROWS],
        ).start()

    def own(ref):
        row = ref[layer : layer + 1, :]
        return jnp.where(core == 0, row[:, :head_size], row[:, head_size:])

    gain = gain_ref[layer : layer + 1, :]
    sums = [None] * (seqs // 16)
    for ref, rows in zip(pieces, piece_rows):
        for at, row in enumerate(rows):
            part = ref[at * 16 : at * 16 + 16, :].astype(jnp.float32)
            scaled_ref[row : row + 16, :] = (part * gain).astype(jnp.bfloat16)
            sums[row // 16] = jnp.sum(part * part, axis=1, keepdims=True)
    projected = lax.dot_general(
        scaled_ref[...],
        weights_ref[...],
        (((1,), (1,)), ((), ())),
        preferred_element_type=jnp.float32,
    )
    at_row = lax.broadcasted_iota(jnp.int32, fold_ref.shape, 0) >> (head_size.bit_length() - 1)
    at_lane = lax.broadcasted_iota(jnp.int32, fold_ref.shape, 1)
    fold_ref[...] = jnp.where(at_row == at_lane, 1.0, 0.0).astype(jnp.bfloat16)
    total = jnp.concatenate(sums, 0)
    projected = projected * lax.rsqrt(total / scaled_ref.shape[1] + RMS_EPS)
    r, k, v, p, q, g = [projected[:, at * head_size : (at + 1) * head_size] for at in range(6)]
    decay = jnp.exp(jax.nn.sigmoid(own(bias_ref) + p) * (-(2.718281828459045**-0.5)))
    rate = jax.nn.sigmoid(q)
    kn = k * lax.rsqrt(jnp.sum(k * k, -1, keepdims=True) + 1.0)
    decay_r = decay * r
    twice = lambda part: jnp.concatenate([part, part], 1)
    kn_wide, decay_r_wide = twice(kn), twice(decay_r)
    repeats = columns // wide
    removed, kept = [], []
    for block in range(seqs // STATE_ROWS):
        span = slice(block * STATE_ROWS, (block + 1) * STATE_ROWS)
        pltpu.make_async_copy(
            state_ref.at[layer, 0, :STATE_ROWS], rows_ref.at[span], arrived.at[block]
        ).wait()
        rows = rows_ref[span, :]
        by_kn = (rows * jnp.tile(kn_wide[span], (1, repeats))).astype(jnp.bfloat16)
        by_r = (rows * jnp.tile(decay_r_wide[span], (1, repeats))).astype(jnp.bfloat16)
        both = jnp.dot(
            jnp.concatenate([by_kn, by_r], 0), fold_ref[...], preferred_element_type=jnp.float32
        )
        removed.append(both[:STATE_ROWS, :head_size])
        kept.append(both[STATE_ROWS:, :head_size])
    removed, kept = jnp.concatenate(removed, 0), jnp.concatenate(kept, 0)
    kn_rate = kn * rate
    k_rate = k * rate
    row_sum = lambda part: jnp.sum(part, -1, keepdims=True)
    readout = kept - removed * row_sum(kn_rate * r) + v * row_sum(k_rate * r)
    center = jnp.mean(readout, -1, keepdims=True)
    spread = jnp.mean(jnp.square(readout - center), -1, keepdims=True)
    normed = (readout - center) * lax.rsqrt(spread + GROUP_EPS) * own(readout_ref)
    out = (normed + row_sum(r * k * own(self_ref)) * v) * jax.nn.sigmoid(g)
    out_ref[...] = out.astype(jnp.bfloat16)
    for at, pair in enumerate(
        (twice(decay), twice(kn_rate), twice(k_rate), jnp.concatenate([v, removed], 1))
    ):
        vec_ref[:, at * wide : (at + 1) * wide] = pair


def front(place, pieces, piece_rows, gain, tables, packed, state, layer):
    seqs, columns = state.shape[2:]
    head_size = packed.shape[0] // 6
    wide = 2 * head_size
    seq_tile = seqs // lax.axis_size("tp")
    whole = lambda shape: pl.BlockSpec(shape, lambda i, s: (0,) * len(shape))
    return pl.pallas_call(
        lambda *refs: front_kernel(
            *refs, piece_rows=piece_rows, seq_tile=seq_tile, head_size=head_size, layer=layer
        ),
        name="front%d" % layer,
        grid_spec=pltpu.PrefetchScalarGridSpec(
            num_scalar_prefetch=1,
            grid=(1,),
            in_specs=[whole(piece.shape) for piece in pieces]
            + [whole(gain.shape)]
            + [pl.BlockSpec((t.shape[0], wide), lambda i, s: (0, s[0])) for t in tables]
            + [whole(packed.shape), pl.BlockSpec(memory_space=pltpu.HBM)],
            out_specs=[whole((seqs, head_size)), whole((seqs, 4 * wide))],
            scratch_shapes=[
                pltpu.VMEM((seqs, D), jnp.bfloat16),
                pltpu.VMEM((columns, wide), jnp.bfloat16),
                pltpu.VMEM((seqs, columns), jnp.float32),
                pltpu.SemaphoreType.DMA((seqs // STATE_ROWS,)),
            ],
        ),
        out_shape=[
            jax.ShapeDtypeStruct((seqs, head_size), jnp.bfloat16),
            jax.ShapeDtypeStruct((seqs, 4 * wide), jnp.float32),
        ],
        compiler_params=pltpu.CompilerParams(vmem_limit_bytes=52 << 20),
    )(place, *pieces, gain, *tables, packed, state)


def update_kernel(place_ref, vec_ref, state_ref, *refs, seq_tile, head_size, layer):
    out_ref, spread_ref, rows_ref, results_ref, arrived, written = refs[-6:]
    wide = 2 * head_size
    seqs, columns = rows_ref.shape
    repeats = columns // wide
    tiles = list(slots(place_ref, seqs, seq_tile))
    for slot, at in enumerate(tiles):
        pltpu.make_async_copy(
            state_ref.at[layer, 0, pl.ds(at, seq_tile)],
            rows_ref.at[slot * seq_tile : (slot + 1) * seq_tile],
            arrived.at[slot * seq_tile // STATE_ROWS],
        ).start()
    at_row = lax.broadcasted_iota(jnp.int32, spread_ref.shape, 0) & (head_size - 1)
    at_lane = lax.broadcasted_iota(jnp.int32, spread_ref.shape, 1) >> (head_size.bit_length() - 1)
    spread_ref[...] = jnp.where(at_row == at_lane, 1.0, 0.0).astype(jnp.bfloat16)
    per_block = STATE_ROWS // seq_tile
    for block in range(seqs // STATE_ROWS):
        span = slice(block * STATE_ROWS, (block + 1) * STATE_ROWS)
        pair = vec_ref[span, 3 * wide :]
        high = pair.astype(jnp.bfloat16)
        low = (pair - high.astype(jnp.float32)).astype(jnp.bfloat16)

        def spread(at):
            lanes = slice(at * head_size, (at + 1) * head_size)
            both = jnp.concatenate([high[:, lanes], low[:, lanes]], 1)
            return jnp.dot(both, spread_ref[...], preferred_element_type=jnp.float32)

        row = lambda at: jnp.tile(vec_ref[span, at * wide : (at + 1) * wide], (1, repeats))
        pltpu.make_async_copy(
            state_ref.at[layer, 0, :STATE_ROWS], rows_ref.at[span], arrived.at[block]
        ).wait()
        results_ref[span, :] = rows_ref[span, :] * row(0) - spread(1) * row(1) + spread(0) * row(2)
        for slot in range(block * per_block, (block + 1) * per_block):
            pltpu.make_async_copy(
                results_ref.at[slot * seq_tile : (slot + 1) * seq_tile],
                out_ref.at[layer, 0, pl.ds(tiles[slot], seq_tile)],
                written.at[block],
            ).start()
    for block in range(seqs // STATE_ROWS):
        span = slice(block * STATE_ROWS, (block + 1) * STATE_ROWS)
        pltpu.make_async_copy(
            results_ref.at[span], out_ref.at[layer, 0, :STATE_ROWS], written.at[block]
        ).wait()


def update(place, vec, state, previous, layer):
    seqs, columns = state.shape[2:]
    head_size = vec.shape[1] // 8
    seq_tile = seqs // lax.axis_size("tp")
    hbm = pl.BlockSpec(memory_space=pltpu.HBM)
    more = [previous] if previous is not None else []
    return pl.pallas_call(
        lambda *refs: update_kernel(
            *refs, seq_tile=seq_tile, head_size=head_size, layer=layer
        ),
        name="update%d" % layer,
        grid_spec=pltpu.PrefetchScalarGridSpec(
            num_scalar_prefetch=1,
            grid=(1,),
            in_specs=[pl.BlockSpec(vec.shape, lambda i, s: (0, 0)), hbm] + [hbm] * len(more),
            out_specs=hbm,
            scratch_shapes=[
                pltpu.VMEM((2 * head_size, columns), jnp.bfloat16),
                pltpu.VMEM((seqs, columns), jnp.float32),
                pltpu.VMEM((seqs, columns), jnp.float32),
                pltpu.SemaphoreType.DMA((seqs // STATE_ROWS,)),
                pltpu.SemaphoreType.DMA((seqs // STATE_ROWS,)),
            ],
        ),
        out_shape=jax.ShapeDtypeStruct(state.shape, state.dtype),
        input_output_aliases={3: 0} if more else {},
        compiler_params=pltpu.CompilerParams(vmem_limit_bytes=52 << 20),
    )(place, vec, state, *more)


def gather_tiles(tile, levels, during):
    step = CORES * PLANE
    near = jnp.concatenate([tile, moved(tile, step)], 0)
    groups = [near]
    if levels > 2:
        far = [moved(tile, step * apart) for apart in range(2, levels)]
        groups.append(jnp.concatenate(far, 0))
    groups[-1], during = lax.optimization_barrier((groups[-1], during))
    during = load(during) if during[0].ndim == 4 else during
    rows = tile.shape[0]
    pieces, places = [], []
    across = []
    start = 0
    for group in groups:
        got = [moved(group, CORES * q) for q in (3, 1, 2)]
        if not across:
            *got, during = lax.optimization_barrier((*got, during))
        across.append((start, group, got))
        start += group.shape[0]
    half = PLANE * levels * rows
    part = lambda q, at, size: [q * levels * rows + at + r for r in range(0, size, 16)]
    sent = jnp.concatenate(groups, 0)
    first = [r for at, group, _ in across for r in part(0, at, group.shape[0])]
    for at, group, got in across:
        pieces += [group] + got
        places += [part(q, at, group.shape[0]) for q in (0, 3, 1, 2)]
    pieces.append(moved(sent, 1))
    places.append([half + r for r in first])
    for at, group, got in across:
        pieces.append(moved(jnp.concatenate(got, 0), 1))
        places.append([half + r for q in (3, 1, 2) for r in part(q, at, group.shape[0])])
    return pieces, places, during


def sum_tiles(parts, levels, during):
    rows = parts.shape[0] // (PLANE * levels)
    block = levels * rows
    sends = parts.astype(jnp.bfloat16)
    got = [moved(sends[q * block : (q + 1) * block], CORES * q) for q in (3, 1, 2)]
    *got, during = lax.optimization_barrier((*got, during))
    summed = parts[:block] + sum(part.astype(jnp.float32) for part in got)
    sends = summed.astype(jnp.bfloat16)
    got = [
        moved(sends[at * rows : (at + 1) * rows], CORES * PLANE * at) for at in range(1, levels)
    ]
    return summed[:rows] + sum(part.astype(jnp.float32) for part in got), during


def on_device_whole(
    tokens,
    block_norm_gain,
    receptance_weight,
    key_weight,
    value_weight,
    decay_weight,
    learning_rate_weight,
    gate_weight,
    decay_bias_fixed,
    self_token_weight,
    readout_norm_gain,
    output_weight,
    state,
):
    devices = lax.axis_size("tp")
    levels = devices // (CORES * PLANE)
    position = lax.axis_index("tp")
    place = jnp.stack([position // CORES, position % CORES]).astype(jnp.int32)
    weights = [
        jnp.swapaxes(w, 2, 3)
        for w in (
            receptance_weight,
            key_weight,
            value_weight,
            decay_weight,
            learning_rate_weight,
            gate_weight,
        )
    ]
    tables = (decay_bias_fixed, self_token_weight, readout_norm_gain)
    own_out = output_weight[:, 0]
    other_out = moved(own_out, 1)

    packed = tuple(weights)
    tile = tokens[0]
    new_state = None
    for layer in range(state.shape[0]):
        pieces, places, packed = gather_tiles(tile, levels, packed)
        out, vec = front(
            place, pieces, places, block_norm_gain, tables, packed[layer], state, layer
        )
        half = out.shape[0] // CORES
        parts = jnp.dot(out[:half], own_out[layer], preferred_element_type=jnp.float32)
        parts += jnp.dot(
            moved(out[half:], 1), other_out[layer], preferred_element_type=jnp.float32
        )
        parts, vec = lax.optimization_barrier((parts, vec))
        new_state = update(place, vec, state, new_state, layer)
        total, new_state = sum_tiles(parts, levels, new_state)
        tile = (tile.astype(jnp.float32) + total).astype(jnp.bfloat16)
    return (tile[None], new_state)


def on_device(tokens, *rest):
    if tokens.shape[2] == D and lax.axis_size("tp") >= 16:
        return on_device_whole(tokens, *rest)
    return on_device_blocked(tokens, *rest)


def solution(mesh):
    return jax.shard_map(
        on_device,
        mesh=mesh,
        in_specs=(
            P("tp", None, None),
            P(),
            P(None, "tp", None, None),
            P(None, "tp", None, None),
            P(None, "tp", None, None),
            P(None, "tp", None, None),
            P(None, "tp", None, None),
            P(None, "tp", None, None),
            P(),
            P(),
            P(),
            P(None, "tp", None, None),
            P(None, "tp", None, None),
        ),
        out_specs=(P("tp", None, None), P(None, "tp", None, None)),
        check_vma=False,
    )
```

```python
from functools import partial

import jax
import jax.numpy as jnp
from jax import lax
from jax.experimental import pallas as pl
from jax.experimental.pallas import tpu as pltpu
from jax.sharding import PartitionSpec as P


D = 4096


RMS_EPS = 1e-06
GROUP_EPS = 0.00064


def swapped(shard, axis, stride):
    return lax.ppermute(shard, axis, [(i, i ^ 1 << stride) for i in range(lax.axis_size(axis))])


def for_sending(shard):

    def short(part):
        return part.astype(jnp.bfloat16) if part.dtype == jnp.float32 else part

    return jax.tree.map(short, shard)


def recurrent_update(
    layer_state,
    receptance_vector,
    key_vector,
    value_vector,
    decay_logits,
    learning_rate_logits,
    gate_logits,
    decay_constant,
    self_term_scale,
    head_gain_slice,
):
    highest = lax.Precision.HIGHEST
    shrink = jnp.exp(-jnp.exp(-jax.nn.softplus(-(decay_constant + decay_logits)) - 0.5))
    rate = jax.nn.sigmoid(learning_rate_logits)
    normed = key_vector * lax.rsqrt(jnp.sum(key_vector * key_vector, -1, keepdims=True) + 1.0)
    removed = jnp.einsum("...ij,...j->...i", layer_state, normed, precision=highest)
    layer_state = (
        layer_state * shrink[..., None, :]
        - removed[..., :, None] * (normed * rate)[..., None, :]
        + value_vector[..., :, None] * (key_vector * rate)[..., None, :]
    )
    readout = jnp.einsum("...ij,...j->...i", layer_state, receptance_vector, precision=highest)
    center = jnp.mean(readout, -1, keepdims=True)
    spread = jnp.mean(jnp.square(readout - center), -1, keepdims=True)
    normed_output = (readout - center) * lax.rsqrt(spread + GROUP_EPS) * head_gain_slice
    self_term = (
        jnp.sum(receptance_vector * key_vector * self_term_scale, -1, keepdims=True) * value_vector
    )
    return (
        ((normed_output + self_term) * jax.nn.sigmoid(gate_logits)).astype(jnp.bfloat16),
        layer_state,
    )


def double_gather(piece, position, first_bit, count, mover):
    for offset in range(count):
        which_bit = first_bit + offset
        partner = mover(piece, which_bit)
        lower_self = position >> which_bit & 1 == 0
        piece = jnp.where(
            lower_self, jnp.concatenate([piece, partner], 0), jnp.concatenate([partner, piece], 0)
        )
    return piece


def halve_sum(members, position, first_bit, count, mover):
    for offset in reversed(range(count)):
        which_bit = first_bit + offset
        upper_self = position >> which_bit & 1 == 1
        sends = tuple(
            (
                jnp.where(
                    upper_self, member[: member.shape[0] // 2], member[member.shape[0] // 2 :]
                )
                for member in members
            )
        )
        keeps = tuple(
            (
                jnp.where(
                    upper_self, member[member.shape[0] // 2 :], member[: member.shape[0] // 2]
                )
                for member in members
            )
        )
        arrived = mover(sends, which_bit)
        members = tuple((kept + got for kept, got in zip(keeps, arrived)))
    return members


def on_device_blocked(
    tokens,
    block_norm_gain,
    receptance_weight,
    key_weight,
    value_weight,
    decay_weight,
    learning_rate_weight,
    gate_weight,
    decay_bias_fixed,
    self_token_weight,
    readout_norm_gain,
    output_weight,
    state,
):
    columns_dev = tokens.shape[2]
    row_blocks = D // columns_dev
    low_bits = row_blocks.bit_length() - 1
    head_count = lax.axis_size("tp") // row_blocks
    high_bits = head_count.bit_length() - 1
    position = lax.axis_index("tp")
    head_index = position // row_blocks
    row_block = position % row_blocks
    head_size = receptance_weight.shape[3]
    seq_tile = tokens.shape[1]
    move_rows = lambda payload, which_bit: swapped(payload, "tp", which_bit)
    move_proj = lambda payload, which_bit: swapped(payload, "tp", which_bit)
    move_outs = lambda payload, which_bit: jax.tree.map(
        lambda part, own: part.astype(own.dtype),
        swapped(for_sending(payload), "tp", which_bit),
        payload,
    )
    move_split = lambda payload, which_bit: jax.tree.map(
        lambda part, own: part.astype(own.dtype),
        swapped(for_sending(payload), "tp", which_bit),
        payload,
    )

    def mixer(columns, layer_index):
        gain_cols = lax.dynamic_slice_in_dim(
            block_norm_gain[layer_index], row_block * columns_dev, columns_dev
        )
        wide = columns.astype(jnp.float32)
        scaled = (wide * gain_cols).astype(jnp.bfloat16)
        squares = jnp.sum(wide * wide, axis=1)
        weights = jnp.concatenate(
            [
                receptance_weight[layer_index, 0],
                key_weight[layer_index, 0],
                value_weight[layer_index, 0],
                decay_weight[layer_index, 0],
                learning_rate_weight[layer_index, 0],
                gate_weight[layer_index, 0],
            ],
            axis=1,
        )
        partial_value = jnp.dot(scaled, weights, preferred_element_type=jnp.float32)
        summed, total_sq = halve_sum((partial_value, squares), position, 0, low_bits, move_proj)
        projected = summed * lax.rsqrt(total_sq / D + RMS_EPS)[:, None]
        output_pieces = jnp.split(projected, 6, axis=1)

        def head_columns(table):
            return lax.dynamic_slice_in_dim(table[layer_index], head_index * head_size, head_size)

        layer_state = state[layer_index, 0].reshape(-1, head_size, head_size)
        out_tile, layer_state = recurrent_update(
            layer_state,
            *output_pieces,
            head_columns(decay_bias_fixed),
            head_columns(self_token_weight),
            head_columns(readout_norm_gain)
        )
        out_all = double_gather(out_tile, position, 0, low_bits, move_outs)
        branch = jnp.dot(out_all, output_weight[layer_index, 0], preferred_element_type=jnp.float32)
        return (branch, layer_state.reshape(layer_state.shape[0], head_size * head_size))

    columns = double_gather(tokens[0], position, low_bits, high_bits, move_rows)
    first_branch, first_memory = mixer(columns, 0)
    (tile_sum,) = halve_sum((first_branch,), position, low_bits, high_bits, move_split)
    tile_one = (tokens[0].astype(jnp.float32) + tile_sum).astype(jnp.bfloat16)
    columns = double_gather(tile_one, position, low_bits, high_bits, move_rows)
    second_branch, second_memory = mixer(columns, 1)
    (tile_sum,) = halve_sum((second_branch,), position, low_bits, high_bits, move_split)
    resid_rows = lax.dynamic_slice_in_dim(columns, head_index * seq_tile, seq_tile, 0)
    mixed = (resid_rows.astype(jnp.float32) + tile_sum).astype(jnp.bfloat16)
    new_state = jnp.stack([first_memory, second_memory])[:, None]
    return (mixed[None], new_state)


CORES = 2
PLANE = 4
STATE_ROWS = 64


def moved(part, mask):
    return lax.ppermute(part, "tp", [(i, i ^ mask) for i in range(lax.axis_size("tp"))])


def near(part):
    return pltpu.with_memory_space_constraint(part, pltpu.VMEM)


def far(part):
    return pltpu.with_memory_space_constraint(part, pltpu.HBM)


def slots(place_ref, rows, seq_tile):
    chips = rows // seq_tile // CORES
    levels = chips // PLANE
    for off_core in range(CORES):
        for apart in range(PLANE):
            for level in range(levels):
                chip = place_ref[0] ^ (apart + PLANE * level)
                tile = chip * CORES + (place_ref[1] ^ off_core)
                yield pl.multiple_of(tile * seq_tile, seq_tile)


def load_kernel(place_ref, *refs, layer, layers, count, head_size, seq_tile):
    arrived, loaded = refs[-2:]
    refs = refs[:-2]
    split = (len(refs) + count - (layers if count else 0)) // 2
    (state_ref, *sources), (rows_ref, *targets) = refs[:split], refs[split:]
    pairs = [
        (ref.at[at_layer, 0], targets[at_layer].at[at * head_size : (at + 1) * head_size, :])
        for at_layer in range(layers if count else 0)
        for at, ref in enumerate(sources[:count])
    ] + list(zip(sources[count:], targets[layers:]))
    copies = [
        pltpu.make_async_copy(source, target, arrived.at[at])
        for at, (source, target) in enumerate(pairs)
    ]
    for copy in copies:
        copy.start()
    for slot, at in enumerate(slots(place_ref, rows_ref.shape[0], seq_tile)):
        pltpu.make_async_copy(
            state_ref.at[layer, 0, pl.ds(at, seq_tile)],
            rows_ref.at[slot * seq_tile : (slot + 1) * seq_tile],
            loaded,
        ).start()
    for copy in copies:
        copy.wait()
    pltpu.make_async_copy(state_ref.at[layer, 0], rows_ref, loaded).wait()


def load(place, state, layer, weights=(), tables=()):
    layers = state.shape[0]
    seqs = state.shape[2]
    outs = [pltpu.VMEM(state.shape[2:], state.dtype)]
    head_size = 0
    if weights:
        _, _, head_size, columns = weights[0].shape
        outs += [pltpu.VMEM((len(weights) * head_size, columns), jnp.bfloat16)] * layers
    outs += [pltpu.VMEM(table.shape, table.dtype) for table in tables]
    sources = [state, *weights, *tables]
    loaded = pl.pallas_call(
        partial(
            load_kernel,
            layer=layer,
            layers=layers,
            count=len(weights),
            head_size=head_size,
            seq_tile=seqs // lax.axis_size("tp"),
        ),
        in_specs=[pl.BlockSpec(memory_space=pltpu.SMEM)]
        + [pl.BlockSpec(memory_space=pltpu.HBM)] * len(sources),
        out_specs=[pl.BlockSpec(memory_space=pltpu.VMEM)] * len(outs),
        out_shape=outs,
        scratch_shapes=[
            pltpu.SemaphoreType.DMA((layers * len(weights) + len(tables) + 1,)),
            pltpu.SemaphoreType.DMA,
        ],
        compiler_params=pltpu.CompilerParams(vmem_limit_bytes=1 << 20),
    )(place, *[far(source) for source in sources])
    return tuple(loaded)


def front_kernel(place_ref, *refs, piece_rows, head_size, layer):
    pieces = refs[: len(piece_rows)]
    (
        gain_ref,
        bias_ref,
        self_ref,
        readout_ref,
        weights_ref,
        rows_ref,
        out_ref,
        vec_ref,
        scaled_ref,
        fold_ref,
    ) = refs[len(piece_rows) :]
    wide = 2 * head_size
    seqs, columns = rows_ref.shape
    core = place_ref[1]

    def own(ref):
        row = ref[layer : layer + 1, pl.ds(pl.multiple_of(place_ref[0] * wide, wide), wide)]
        return jnp.where(core == 0, row[:, :head_size], row[:, head_size:])

    gain = gain_ref[layer : layer + 1, :]
    sums = [None] * (seqs // 16)
    for ref, rows in zip(pieces, piece_rows):
        for at, row in enumerate(rows):
            part = ref[at * 16 : at * 16 + 16, :].astype(jnp.float32)
            scaled_ref[row : row + 16, :] = (part * gain).astype(jnp.bfloat16)
            sums[row // 16] = jnp.sum(part * part, axis=1, keepdims=True)
    projected = lax.dot_general(
        scaled_ref[...],
        weights_ref[...],
        (((1,), (1,)), ((), ())),
        preferred_element_type=jnp.float32,
    )
    at_row = lax.broadcasted_iota(jnp.int32, fold_ref.shape, 0) >> (head_size.bit_length() - 1)
    at_lane = lax.broadcasted_iota(jnp.int32, fold_ref.shape, 1)
    fold_ref[...] = jnp.where(at_row == at_lane, 1.0, 0.0).astype(jnp.bfloat16)
    total = jnp.concatenate(sums, 0)
    projected = projected * lax.rsqrt(total / scaled_ref.shape[1] + RMS_EPS)
    r, k, v, p, q, g = [projected[:, at * head_size : (at + 1) * head_size] for at in range(6)]
    decay = jnp.exp(jax.nn.sigmoid(own(bias_ref) + p) * (-(2.718281828459045**-0.5)))
    rate = jax.nn.sigmoid(q)
    kn = k * lax.rsqrt(jnp.sum(k * k, -1, keepdims=True) + 1.0)
    decay_r = decay * r
    twice = lambda part: jnp.concatenate([part, part], 1)
    kn_wide, decay_r_wide = twice(kn), twice(decay_r)
    repeats = columns // wide
    removed, kept = [], []
    for block in range(seqs // STATE_ROWS):
        span = slice(block * STATE_ROWS, (block + 1) * STATE_ROWS)
        rows = rows_ref[span, :]
        by_kn = (rows * jnp.tile(kn_wide[span], (1, repeats))).astype(jnp.bfloat16)
        by_r = (rows * jnp.tile(decay_r_wide[span], (1, repeats))).astype(jnp.bfloat16)
        both = jnp.dot(
            jnp.concatenate([by_kn, by_r], 0), fold_ref[...], preferred_element_type=jnp.float32
        )
        removed.append(both[:STATE_ROWS, :head_size])
        kept.append(both[STATE_ROWS:, :head_size])
    removed, kept = jnp.concatenate(removed, 0), jnp.concatenate(kept, 0)
    kn_rate = kn * rate
    k_rate = k * rate
    row_sum = lambda part: jnp.sum(part, -1, keepdims=True)
    readout = kept - removed * row_sum(kn_rate * r) + v * row_sum(k_rate * r)
    center = jnp.mean(readout, -1, keepdims=True)
    spread = jnp.mean(jnp.square(readout - center), -1, keepdims=True)
    normed = (readout - center) * lax.rsqrt(spread + GROUP_EPS) * own(readout_ref)
    out = (normed + row_sum(r * k * own(self_ref)) * v) * jax.nn.sigmoid(g)
    out_ref[...] = out.astype(jnp.bfloat16)
    for at, pair in enumerate(
        (twice(decay), twice(kn_rate), twice(k_rate), jnp.concatenate([v, removed], 1))
    ):
        vec_ref[:, at * wide : (at + 1) * wide] = pair


def front(place, pieces, piece_rows, gain, tables, packed, rows, layer):
    seqs, columns = rows.shape
    head_size = packed.shape[0] // 6
    wide = 2 * head_size
    vmem = pl.BlockSpec(memory_space=pltpu.VMEM)
    return pl.pallas_call(
        partial(front_kernel, piece_rows=piece_rows, head_size=head_size, layer=layer),
        in_specs=[pl.BlockSpec(memory_space=pltpu.SMEM)]
        + [vmem] * (len(pieces) + 3 + len(tables)),
        out_specs=[vmem, vmem],
        scratch_shapes=[
            pltpu.VMEM((seqs, D), jnp.bfloat16),
            pltpu.VMEM((columns, wide), jnp.bfloat16),
        ],
        out_shape=[
            jax.ShapeDtypeStruct((seqs, head_size), jnp.bfloat16),
            jax.ShapeDtypeStruct((seqs, 4 * wide), jnp.float32),
        ],
        compiler_params=pltpu.CompilerParams(vmem_limit_bytes=36 << 20),
    )(place, *[near(piece) for piece in pieces], near(gain), *[near(t) for t in tables], near(packed), near(rows))


def update_kernel(place_ref, vec_ref, rows_ref, *refs, seq_tile, head_size, layer):
    out_ref, spread_ref, results_ref, written = refs[-4:]
    wide = 2 * head_size
    seqs, columns = rows_ref.shape
    repeats = columns // wide
    at_row = lax.broadcasted_iota(jnp.int32, spread_ref.shape, 0) & (head_size - 1)
    at_lane = lax.broadcasted_iota(jnp.int32, spread_ref.shape, 1) >> (head_size.bit_length() - 1)
    spread_ref[...] = jnp.where(at_row == at_lane, 1.0, 0.0).astype(jnp.bfloat16)
    tiles = list(slots(place_ref, seqs, seq_tile))
    per_block = STATE_ROWS // seq_tile
    for block in range(seqs // STATE_ROWS):
        span = slice(block * STATE_ROWS, (block + 1) * STATE_ROWS)
        pair = vec_ref[span, 3 * wide :]
        high = pair.astype(jnp.bfloat16)
        low = (pair - high.astype(jnp.float32)).astype(jnp.bfloat16)

        def spread(at):
            lanes = slice(at * head_size, (at + 1) * head_size)
            both = jnp.concatenate([high[:, lanes], low[:, lanes]], 1)
            return jnp.dot(both, spread_ref[...], preferred_element_type=jnp.float32)

        row = lambda at: jnp.tile(vec_ref[span, at * wide : (at + 1) * wide], (1, repeats))
        results_ref[span, :] = rows_ref[span, :] * row(0) - spread(1) * row(1) + spread(0) * row(2)
        for slot in range(block * per_block, (block + 1) * per_block):
            pltpu.make_async_copy(
                results_ref.at[slot * seq_tile : (slot + 1) * seq_tile],
                out_ref.at[layer, 0, pl.ds(tiles[slot], seq_tile)],
                written.at[block],
            ).start()
    for block in range(seqs // STATE_ROWS):
        span = slice(block * STATE_ROWS, (block + 1) * STATE_ROWS)
        pltpu.make_async_copy(
            results_ref.at[span], out_ref.at[layer, 0, :STATE_ROWS], written.at[block]
        ).wait()


def update(place, vec, rows, previous, shape, layer):
    seqs, columns = rows.shape
    head_size = vec.shape[1] // 8
    vmem = pl.BlockSpec(memory_space=pltpu.VMEM)
    hbm = pl.BlockSpec(memory_space=pltpu.HBM)
    more = [previous] if previous is not None else []
    return pl.pallas_call(
        partial(
            update_kernel,
            seq_tile=seqs // lax.axis_size("tp"),
            head_size=head_size,
            layer=layer,
        ),
        in_specs=[pl.BlockSpec(memory_space=pltpu.SMEM), vmem, vmem] + [hbm] * len(more),
        out_specs=hbm,
        scratch_shapes=[
            pltpu.VMEM((2 * head_size, columns), jnp.bfloat16),
            pltpu.VMEM((seqs, columns), jnp.float32),
            pltpu.SemaphoreType.DMA((seqs // STATE_ROWS,)),
        ],
        out_shape=jax.ShapeDtypeStruct(shape, rows.dtype),
        input_output_aliases={3: 0} if more else {},
        compiler_params=pltpu.CompilerParams(vmem_limit_bytes=24 << 20),
    )(place, near(vec), near(rows), *more)


def gather_tiles(tile, levels):
    step = CORES * PLANE
    groups = [jnp.concatenate([tile, moved(tile, step)], 0)]
    if levels > 2:
        distant = [moved(tile, step * apart) for apart in range(2, levels)]
        groups.append(jnp.concatenate(distant, 0))
    rows = tile.shape[0]
    half = PLANE * levels * rows
    part = lambda q, at, size: [q * levels * rows + at + r for r in range(0, size, 16)]
    pieces, places, swaps = [], [], []
    start = 0
    for group in groups:
        order = (3, 1, 2)
        got = [moved(group, CORES * q) for q in order]
        pieces += [group] + got
        places += [part(q, start, group.shape[0]) for q in (0, *order)]
        swaps.append((got, [r for q in order for r in part(q, start, group.shape[0])]))
        start += group.shape[0]
    swaps.insert(0, (groups, part(0, 0, start)))
    for parts, spots in swaps:
        pieces.append(moved(jnp.concatenate(parts, 0), 1))
        places.append([half + r for r in spots])
    return pieces, places


def sum_tiles(parts, levels, during):
    rows = parts.shape[0] // (PLANE * levels)
    block = levels * rows
    sends = parts.astype(jnp.bfloat16)
    got = [moved(sends[q * block : (q + 1) * block], CORES * q) for q in (3, 1, 2)]
    *got, during = lax.optimization_barrier((*got, during))
    summed = parts[:block] + sum(part.astype(jnp.float32) for part in got)
    sends = summed.astype(jnp.bfloat16)
    got = [
        moved(sends[at * rows : (at + 1) * rows], CORES * PLANE * at) for at in range(1, levels)
    ]
    return summed[:rows] + sum(part.astype(jnp.float32) for part in got), during


def on_device_whole(
    tokens,
    block_norm_gain,
    receptance_weight,
    key_weight,
    value_weight,
    decay_weight,
    learning_rate_weight,
    gate_weight,
    decay_bias_fixed,
    self_token_weight,
    readout_norm_gain,
    output_weight,
    state,
):
    devices = lax.axis_size("tp")
    levels = devices // (CORES * PLANE)
    position = lax.axis_index("tp")
    place = jnp.stack([position // CORES, position % CORES]).astype(jnp.int32)
    weights = [
        jnp.swapaxes(w, 2, 3)
        for w in (
            receptance_weight,
            key_weight,
            value_weight,
            decay_weight,
            learning_rate_weight,
            gate_weight,
        )
    ]
    tables = (decay_bias_fixed, self_token_weight, readout_norm_gain)
    own_out = output_weight[:, 0]
    other_out = moved(own_out, 1)

    tile, place = lax.optimization_barrier((tokens[0], place))
    new_state = None
    layers = state.shape[0]
    for layer in range(layers):
        pieces, places = gather_tiles(tile, levels)
        if layer == 0:
            loaded = load(place, state, layer, weights, (block_norm_gain, *tables))
            packed, (gain, *tables) = loaded[1 : 1 + layers], loaded[1 + layers :]
        else:
            loaded = load(place, state, layer)
        rows = loaded[0]
        out, vec = front(place, pieces, places, gain, tables, packed[layer], rows, layer)
        half = out.shape[0] // CORES
        parts = jnp.dot(out[:half], own_out[layer], preferred_element_type=jnp.float32)
        parts += jnp.dot(moved(out[half:], 1), other_out[layer], preferred_element_type=jnp.float32)
        parts, vec = lax.optimization_barrier((parts, vec))
        new_state = update(place, vec, rows, new_state, state.shape, layer)
        total, new_state = sum_tiles(parts, levels, new_state)
        tile = (tile.astype(jnp.float32) + total).astype(jnp.bfloat16)
    return (tile[None], new_state)


def on_device(tokens, *rest):
    if tokens.shape[2] == D and lax.axis_size("tp") >= 16:
        return on_device_whole(tokens, *rest)
    return on_device_blocked(tokens, *rest)


def solution(mesh):
    return jax.shard_map(
        on_device,
        mesh=mesh,
        in_specs=(
            P("tp", None, None),
            P(),
            P(None, "tp", None, None),
            P(None, "tp", None, None),
            P(None, "tp", None, None),
            P(None, "tp", None, None),
            P(None, "tp", None, None),
            P(None, "tp", None, None),
            P(),
            P(),
            P(),
            P(None, "tp", None, None),
            P(None, "tp", None, None),
        ),
        out_specs=(P("tp", None, None), P(None, "tp", None, None)),
        check_vma=False,
    )
```

```python
from functools import partial

import jax
import jax.numpy as jnp
from jax import lax
from jax.experimental import pallas as pl
from jax.experimental.pallas import tpu as pltpu
from jax.sharding import PartitionSpec as P


D = 4096


RMS_EPS = 1e-06
GROUP_EPS = 0.00064


def swapped(shard, axis, stride):
    return lax.ppermute(shard, axis, [(i, i ^ 1 << stride) for i in range(lax.axis_size(axis))])


def for_sending(shard):

    def short(part):
        return part.astype(jnp.bfloat16) if part.dtype == jnp.float32 else part

    return jax.tree.map(short, shard)


def recurrent_update(
    layer_state,
    receptance_vector,
    key_vector,
    value_vector,
    decay_logits,
    learning_rate_logits,
    gate_logits,
    decay_constant,
    self_term_scale,
    head_gain_slice,
):
    highest = lax.Precision.HIGHEST
    shrink = jnp.exp(-jnp.exp(-jax.nn.softplus(-(decay_constant + decay_logits)) - 0.5))
    rate = jax.nn.sigmoid(learning_rate_logits)
    normed = key_vector * lax.rsqrt(jnp.sum(key_vector * key_vector, -1, keepdims=True) + 1.0)
    removed = jnp.einsum("...ij,...j->...i", layer_state, normed, precision=highest)
    layer_state = (
        layer_state * shrink[..., None, :]
        - removed[..., :, None] * (normed * rate)[..., None, :]
        + value_vector[..., :, None] * (key_vector * rate)[..., None, :]
    )
    readout = jnp.einsum("...ij,...j->...i", layer_state, receptance_vector, precision=highest)
    center = jnp.mean(readout, -1, keepdims=True)
    spread = jnp.mean(jnp.square(readout - center), -1, keepdims=True)
    normed_output = (readout - center) * lax.rsqrt(spread + GROUP_EPS) * head_gain_slice
    self_term = (
        jnp.sum(receptance_vector * key_vector * self_term_scale, -1, keepdims=True) * value_vector
    )
    return (
        ((normed_output + self_term) * jax.nn.sigmoid(gate_logits)).astype(jnp.bfloat16),
        layer_state,
    )


def double_gather(piece, position, first_bit, count, mover):
    for offset in range(count):
        which_bit = first_bit + offset
        partner = mover(piece, which_bit)
        lower_self = position >> which_bit & 1 == 0
        piece = jnp.where(
            lower_self, jnp.concatenate([piece, partner], 0), jnp.concatenate([partner, piece], 0)
        )
    return piece


def halve_sum(members, position, first_bit, count, mover):
    for offset in reversed(range(count)):
        which_bit = first_bit + offset
        upper_self = position >> which_bit & 1 == 1
        sends = tuple(
            (
                jnp.where(
                    upper_self, member[: member.shape[0] // 2], member[member.shape[0] // 2 :]
                )
                for member in members
            )
        )
        keeps = tuple(
            (
                jnp.where(
                    upper_self, member[member.shape[0] // 2 :], member[: member.shape[0] // 2]
                )
                for member in members
            )
        )
        arrived = mover(sends, which_bit)
        members = tuple((kept + got for kept, got in zip(keeps, arrived)))
    return members


def on_device_blocked(
    tokens,
    block_norm_gain,
    receptance_weight,
    key_weight,
    value_weight,
    decay_weight,
    learning_rate_weight,
    gate_weight,
    decay_bias_fixed,
    self_token_weight,
    readout_norm_gain,
    output_weight,
    state,
):
    columns_dev = tokens.shape[2]
    row_blocks = D // columns_dev
    low_bits = row_blocks.bit_length() - 1
    head_count = lax.axis_size("tp") // row_blocks
    high_bits = head_count.bit_length() - 1
    position = lax.axis_index("tp")
    head_index = position // row_blocks
    row_block = position % row_blocks
    head_size = receptance_weight.shape[3]
    seq_tile = tokens.shape[1]
    move_rows = lambda payload, which_bit: swapped(payload, "tp", which_bit)
    move_proj = lambda payload, which_bit: swapped(payload, "tp", which_bit)
    move_outs = lambda payload, which_bit: jax.tree.map(
        lambda part, own: part.astype(own.dtype),
        swapped(for_sending(payload), "tp", which_bit),
        payload,
    )
    move_split = lambda payload, which_bit: jax.tree.map(
        lambda part, own: part.astype(own.dtype),
        swapped(for_sending(payload), "tp", which_bit),
        payload,
    )

    def mixer(columns, layer_index):
        gain_cols = lax.dynamic_slice_in_dim(
            block_norm_gain[layer_index], row_block * columns_dev, columns_dev
        )
        wide = columns.astype(jnp.float32)
        scaled = (wide * gain_cols).astype(jnp.bfloat16)
        squares = jnp.sum(wide * wide, axis=1)
        weights = jnp.concatenate(
            [
                receptance_weight[layer_index, 0],
                key_weight[layer_index, 0],
                value_weight[layer_index, 0],
                decay_weight[layer_index, 0],
                learning_rate_weight[layer_index, 0],
                gate_weight[layer_index, 0],
            ],
            axis=1,
        )
        partial_value = jnp.dot(scaled, weights, preferred_element_type=jnp.float32)
        summed, total_sq = halve_sum((partial_value, squares), position, 0, low_bits, move_proj)
        projected = summed * lax.rsqrt(total_sq / D + RMS_EPS)[:, None]
        output_pieces = jnp.split(projected, 6, axis=1)

        def head_columns(table):
            return lax.dynamic_slice_in_dim(table[layer_index], head_index * head_size, head_size)

        layer_state = state[layer_index, 0].reshape(-1, head_size, head_size)
        out_tile, layer_state = recurrent_update(
            layer_state,
            *output_pieces,
            head_columns(decay_bias_fixed),
            head_columns(self_token_weight),
            head_columns(readout_norm_gain)
        )
        out_all = double_gather(out_tile, position, 0, low_bits, move_outs)
        branch = jnp.dot(out_all, output_weight[layer_index, 0], preferred_element_type=jnp.float32)
        return (branch, layer_state.reshape(layer_state.shape[0], head_size * head_size))

    columns = double_gather(tokens[0], position, low_bits, high_bits, move_rows)
    first_branch, first_memory = mixer(columns, 0)
    (tile_sum,) = halve_sum((first_branch,), position, low_bits, high_bits, move_split)
    tile_one = (tokens[0].astype(jnp.float32) + tile_sum).astype(jnp.bfloat16)
    columns = double_gather(tile_one, position, low_bits, high_bits, move_rows)
    second_branch, second_memory = mixer(columns, 1)
    (tile_sum,) = halve_sum((second_branch,), position, low_bits, high_bits, move_split)
    resid_rows = lax.dynamic_slice_in_dim(columns, head_index * seq_tile, seq_tile, 0)
    mixed = (resid_rows.astype(jnp.float32) + tile_sum).astype(jnp.bfloat16)
    new_state = jnp.stack([first_memory, second_memory])[:, None]
    return (mixed[None], new_state)


CORES = 2
PLANE = 4
STATE_ROWS = 64


def moved(part, mask):
    return lax.ppermute(part, "tp", [(i, i ^ mask) for i in range(lax.axis_size("tp"))])


def near(part):
    return pltpu.with_memory_space_constraint(part, pltpu.VMEM)


def far(part):
    return pltpu.with_memory_space_constraint(part, pltpu.HBM)


def slots(place_ref, rows, seq_tile):
    chips = rows // seq_tile // CORES
    levels = chips // PLANE
    for off_core in range(CORES):
        for apart in range(PLANE):
            for level in range(levels):
                chip = place_ref[0] ^ (apart + PLANE * level)
                tile = chip * CORES + (place_ref[1] ^ off_core)
                yield pl.multiple_of(tile * seq_tile, seq_tile)


def load_kernel(place_ref, *refs, layer, layers, count, head_size, seq_tile):
    arrived, loaded = refs[-2:]
    refs = refs[:-2]
    split = (len(refs) + count - (layers if count else 0)) // 2
    (state_ref, *sources), (rows_ref, *targets) = refs[:split], refs[split:]
    pairs = [
        (ref.at[at_layer, 0], targets[at_layer].at[at * head_size : (at + 1) * head_size, :])
        for at_layer in range(layers if count else 0)
        for at, ref in enumerate(sources[:count])
    ] + list(zip(sources[count:], targets[layers:]))
    copies = [
        pltpu.make_async_copy(source, target, arrived.at[at])
        for at, (source, target) in enumerate(pairs)
    ]
    for copy in copies:
        copy.start()
    for slot, at in enumerate(slots(place_ref, rows_ref.shape[0], seq_tile)):
        pltpu.make_async_copy(
            state_ref.at[layer, 0, pl.ds(at, seq_tile)],
            rows_ref.at[slot * seq_tile : (slot + 1) * seq_tile],
            loaded,
        ).start()
    for copy in copies:
        copy.wait()
    pltpu.make_async_copy(state_ref.at[layer, 0], rows_ref, loaded).wait()


def load(place, state, layer, weights=(), tables=()):
    layers = state.shape[0]
    seqs = state.shape[2]
    outs = [pltpu.VMEM(state.shape[2:], state.dtype)]
    head_size = 0
    if weights:
        _, _, head_size, columns = weights[0].shape
        outs += [pltpu.VMEM((len(weights) * head_size, columns), jnp.bfloat16)] * layers
    outs += [pltpu.VMEM(table.shape, table.dtype) for table in tables]
    sources = [state, *weights, *tables]
    loaded = pl.pallas_call(
        partial(
            load_kernel,
            layer=layer,
            layers=layers,
            count=len(weights),
            head_size=head_size,
            seq_tile=seqs // lax.axis_size("tp"),
        ),
        in_specs=[pl.BlockSpec(memory_space=pltpu.SMEM)]
        + [pl.BlockSpec(memory_space=pltpu.HBM)] * len(sources),
        out_specs=[pl.BlockSpec(memory_space=pltpu.VMEM)] * len(outs),
        out_shape=outs,
        scratch_shapes=[
            pltpu.SemaphoreType.DMA((layers * len(weights) + len(tables) + 1,)),
            pltpu.SemaphoreType.DMA,
        ],
        compiler_params=pltpu.CompilerParams(vmem_limit_bytes=1 << 20),
    )(place, *[far(source) for source in sources])
    return tuple(loaded)


def front_kernel(place_ref, *refs, piece_rows, head_size, layer):
    pieces = refs[: len(piece_rows)]
    (
        gain_ref,
        bias_ref,
        self_ref,
        readout_ref,
        weights_ref,
        rows_ref,
        out_ref,
        vec_ref,
        scaled_ref,
        fold_ref,
    ) = refs[len(piece_rows) :]
    wide = 2 * head_size
    seqs, columns = rows_ref.shape
    core = place_ref[1]

    def own(ref):
        row = ref[layer : layer + 1, pl.ds(pl.multiple_of(place_ref[0] * wide, wide), wide)]
        return jnp.where(core == 0, row[:, :head_size], row[:, head_size:])

    gain = gain_ref[layer : layer + 1, :]
    sums = [None] * (seqs // 16)
    for ref, rows in zip(pieces, piece_rows):
        for at, row in enumerate(rows):
            part = ref[at * 16 : at * 16 + 16, :].astype(jnp.float32)
            scaled_ref[row : row + 16, :] = (part * gain).astype(jnp.bfloat16)
            sums[row // 16] = jnp.sum(part * part, axis=1, keepdims=True)
    projected = lax.dot_general(
        scaled_ref[...],
        weights_ref[...],
        (((1,), (1,)), ((), ())),
        preferred_element_type=jnp.float32,
    )
    at_row = lax.broadcasted_iota(jnp.int32, fold_ref.shape, 0) >> (head_size.bit_length() - 1)
    at_lane = lax.broadcasted_iota(jnp.int32, fold_ref.shape, 1)
    fold_ref[...] = jnp.where(at_row == at_lane, 1.0, 0.0).astype(jnp.bfloat16)
    total = jnp.concatenate(sums, 0)
    projected = projected * lax.rsqrt(total / scaled_ref.shape[1] + RMS_EPS)
    r, k, v, p, q, g = [projected[:, at * head_size : (at + 1) * head_size] for at in range(6)]
    decay = jnp.exp(jax.nn.sigmoid(own(bias_ref) + p) * (-(2.718281828459045**-0.5)))
    rate = jax.nn.sigmoid(q)
    kn = k * lax.rsqrt(jnp.sum(k * k, -1, keepdims=True) + 1.0)
    decay_r = decay * r
    twice = lambda part: jnp.concatenate([part, part], 1)
    kn_wide, decay_r_wide = twice(kn), twice(decay_r)
    repeats = columns // wide
    removed, kept = [], []
    for block in range(seqs // STATE_ROWS):
        span = slice(block * STATE_ROWS, (block + 1) * STATE_ROWS)
        rows = rows_ref[span, :]
        by_kn = (rows * jnp.tile(kn_wide[span], (1, repeats))).astype(jnp.bfloat16)
        by_r = (rows * jnp.tile(decay_r_wide[span], (1, repeats))).astype(jnp.bfloat16)
        both = jnp.dot(
            jnp.concatenate([by_kn, by_r], 0), fold_ref[...], preferred_element_type=jnp.float32
        )
        removed.append(both[:STATE_ROWS, :head_size])
        kept.append(both[STATE_ROWS:, :head_size])
    removed, kept = jnp.concatenate(removed, 0), jnp.concatenate(kept, 0)
    kn_rate = kn * rate
    k_rate = k * rate
    row_sum = lambda part: jnp.sum(part, -1, keepdims=True)
    readout = kept - removed * row_sum(kn_rate * r) + v * row_sum(k_rate * r)
    center = jnp.mean(readout, -1, keepdims=True)
    spread = jnp.mean(jnp.square(readout - center), -1, keepdims=True)
    normed = (readout - center) * lax.rsqrt(spread + GROUP_EPS) * own(readout_ref)
    out = (normed + row_sum(r * k * own(self_ref)) * v) * jax.nn.sigmoid(g)
    out_ref[...] = out.astype(jnp.bfloat16)
    for at, pair in enumerate(
        (twice(decay), twice(kn_rate), twice(k_rate), jnp.concatenate([v, removed], 1))
    ):
        vec_ref[:, at * wide : (at + 1) * wide] = pair


def front(place, pieces, piece_rows, gain, tables, packed, rows, layer):
    seqs, columns = rows.shape
    head_size = packed.shape[0] // 6
    wide = 2 * head_size
    vmem = pl.BlockSpec(memory_space=pltpu.VMEM)
    return pl.pallas_call(
        partial(front_kernel, piece_rows=piece_rows, head_size=head_size, layer=layer),
        in_specs=[pl.BlockSpec(memory_space=pltpu.SMEM)]
        + [vmem] * (len(pieces) + 3 + len(tables)),
        out_specs=[vmem, vmem],
        scratch_shapes=[
            pltpu.VMEM((seqs, D), jnp.bfloat16),
            pltpu.VMEM((columns, wide), jnp.bfloat16),
        ],
        out_shape=[
            jax.ShapeDtypeStruct((seqs, head_size), jnp.bfloat16),
            jax.ShapeDtypeStruct((seqs, 4 * wide), jnp.float32),
        ],
        compiler_params=pltpu.CompilerParams(vmem_limit_bytes=36 << 20),
    )(place, *[near(piece) for piece in pieces], near(gain), *[near(t) for t in tables], near(packed), near(rows))


def update_kernel(place_ref, vec_ref, rows_ref, *refs, seq_tile, head_size, layer, part):
    out_ref, spread_ref, results_ref, written = refs[-4:]
    wide = 2 * head_size
    seqs, columns = rows_ref.shape
    repeats = columns // wide
    at_row = lax.broadcasted_iota(jnp.int32, spread_ref.shape, 0) & (head_size - 1)
    at_lane = lax.broadcasted_iota(jnp.int32, spread_ref.shape, 1) >> (head_size.bit_length() - 1)
    spread_ref[...] = jnp.where(at_row == at_lane, 1.0, 0.0).astype(jnp.bfloat16)
    tiles = list(slots(place_ref, seqs, seq_tile))
    per_block = STATE_ROWS // seq_tile
    blocks = seqs // STATE_ROWS // CORES
    blocks = range(part * blocks, (part + 1) * blocks)
    for block in blocks:
        span = slice(block * STATE_ROWS, (block + 1) * STATE_ROWS)
        local = slice(
            (block - blocks[0]) * STATE_ROWS, (block - blocks[0] + 1) * STATE_ROWS
        )
        pair = vec_ref[span, 3 * wide :]
        high = pair.astype(jnp.bfloat16)
        low = (pair - high.astype(jnp.float32)).astype(jnp.bfloat16)

        def spread(at):
            lanes = slice(at * head_size, (at + 1) * head_size)
            both = jnp.concatenate([high[:, lanes], low[:, lanes]], 1)
            return jnp.dot(both, spread_ref[...], preferred_element_type=jnp.float32)

        row = lambda at: jnp.tile(vec_ref[span, at * wide : (at + 1) * wide], (1, repeats))
        results_ref[local, :] = rows_ref[span, :] * row(0) - spread(1) * row(1) + spread(0) * row(2)
        for slot in range(block * per_block, (block + 1) * per_block):
            at = slot * seq_tile - blocks[0] * STATE_ROWS
            pltpu.make_async_copy(
                results_ref.at[at : at + seq_tile],
                out_ref.at[layer, 0, pl.ds(tiles[slot], seq_tile)],
                written.at[block - blocks[0]],
            ).start()
    for at in range(len(blocks)):
        span = slice(at * STATE_ROWS, (at + 1) * STATE_ROWS)
        pltpu.make_async_copy(
            results_ref.at[span], out_ref.at[layer, 0, :STATE_ROWS], written.at[at]
        ).wait()


def update(place, vec, rows, previous, shape, layer, part):
    seqs, columns = rows.shape
    head_size = vec.shape[1] // 8
    vmem = pl.BlockSpec(memory_space=pltpu.VMEM)
    hbm = pl.BlockSpec(memory_space=pltpu.HBM)
    more = [previous] if previous is not None else []
    return pl.pallas_call(
        partial(
            update_kernel,
            seq_tile=seqs // lax.axis_size("tp"),
            head_size=head_size,
            layer=layer,
            part=part,
        ),
        in_specs=[pl.BlockSpec(memory_space=pltpu.SMEM), vmem, vmem] + [hbm] * len(more),
        out_specs=hbm,
        scratch_shapes=[
            pltpu.VMEM((2 * head_size, columns), jnp.bfloat16),
            pltpu.VMEM((seqs // CORES, columns), jnp.float32),
            pltpu.SemaphoreType.DMA((seqs // STATE_ROWS // CORES,)),
        ],
        out_shape=jax.ShapeDtypeStruct(shape, rows.dtype),
        input_output_aliases={3: 0} if more else {},
        compiler_params=pltpu.CompilerParams(vmem_limit_bytes=24 << 20),
    )(place, near(vec), near(rows), *more)


def gather_tiles(tile, levels):
    step = CORES * PLANE
    corner = moved(tile, CORES * 3)
    column = {at: moved(tile, step * at) for at in range(1, levels)}
    corners = {at: moved(corner, step * at) for at in range(1, levels)}
    column = jnp.concatenate([tile, *column.values()], 0)
    across = [moved(column, CORES * q) for q in (1, 2)]
    corners = jnp.concatenate([corner, *corners.values()], 0)
    pieces = [column, *across, corners]
    pieces += [moved(piece, 1) for piece in pieces]
    block = column.shape[0]
    places = [[at * block + r for r in range(0, block, 16)] for at in range(len(pieces))]
    return pieces, places


def sum_tiles(parts, levels, new_state, update_part):
    rows = parts.shape[0] // (PLANE * levels)
    block = levels * rows
    step = CORES * PLANE
    wide = lambda got: [part.astype(jnp.float32) for part in got]
    sends = parts.astype(jnp.bfloat16)
    across = [moved(sends[q * block : (q + 1) * block], CORES * q) for q in (1, 2)]
    diagonal = sends[3 * block :]
    along = [moved(diagonal[at * rows : (at + 1) * rows], step * at) for at in range(1, levels)]
    new_state = update_part(new_state, 0)
    *across, new_state = lax.optimization_barrier((*across, new_state))
    summed = parts[:block] + sum(wide(across))
    sends = summed.astype(jnp.bfloat16)
    got = [moved(sends[at * rows : (at + 1) * rows], step * at) for at in range(1, levels)]
    corner = (parts[3 * block : 3 * block + rows] + sum(wide(along))).astype(jnp.bfloat16)
    got.append(moved(corner, CORES * 3))
    new_state = update_part(new_state, 1)
    *got, new_state = lax.optimization_barrier((*got, new_state))
    return summed[:rows] + sum(wide(got)), new_state


def on_device_whole(
    tokens,
    block_norm_gain,
    receptance_weight,
    key_weight,
    value_weight,
    decay_weight,
    learning_rate_weight,
    gate_weight,
    decay_bias_fixed,
    self_token_weight,
    readout_norm_gain,
    output_weight,
    state,
):
    devices = lax.axis_size("tp")
    levels = devices // (CORES * PLANE)
    position = lax.axis_index("tp")
    place = jnp.stack([position // CORES, position % CORES]).astype(jnp.int32)
    weights = [
        jnp.swapaxes(w, 2, 3)
        for w in (
            receptance_weight,
            key_weight,
            value_weight,
            decay_weight,
            learning_rate_weight,
            gate_weight,
        )
    ]
    tables = (decay_bias_fixed, self_token_weight, readout_norm_gain)
    own_out = output_weight[:, 0]
    other_out = moved(own_out, 1)

    tile, place = lax.optimization_barrier((tokens[0], place))
    new_state = None
    layers = state.shape[0]
    for layer in range(layers):
        pieces, places = gather_tiles(tile, levels)
        if layer == 0:
            loaded = load(place, state, layer, weights, (block_norm_gain, *tables))
            packed, (gain, *tables) = loaded[1 : 1 + layers], loaded[1 + layers :]
        else:
            loaded = load(place, state, layer)
        rows = loaded[0]
        out, vec = front(place, pieces, places, gain, tables, packed[layer], rows, layer)
        half = out.shape[0] // CORES
        parts = jnp.dot(out[:half], own_out[layer], preferred_element_type=jnp.float32)
        parts += jnp.dot(moved(out[half:], 1), other_out[layer], preferred_element_type=jnp.float32)
        parts, vec = lax.optimization_barrier((parts, vec))
        update_part = lambda previous, part: update(
            place, vec, rows, previous, state.shape, layer, part
        )
        total, new_state = sum_tiles(parts, levels, new_state, update_part)
        tile = (tile.astype(jnp.float32) + total).astype(jnp.bfloat16)
    return (tile[None], new_state)


def on_device(tokens, *rest):
    if tokens.shape[2] == D and lax.axis_size("tp") >= 16:
        return on_device_whole(tokens, *rest)
    return on_device_blocked(tokens, *rest)


def solution(mesh):
    return jax.shard_map(
        on_device,
        mesh=mesh,
        in_specs=(
            P("tp", None, None),
            P(),
            P(None, "tp", None, None),
            P(None, "tp", None, None),
            P(None, "tp", None, None),
            P(None, "tp", None, None),
            P(None, "tp", None, None),
            P(None, "tp", None, None),
            P(),
            P(),
            P(),
            P(None, "tp", None, None),
            P(None, "tp", None, None),
        ),
        out_specs=(P("tp", None, None), P(None, "tp", None, None)),
        check_vma=False,
    )
```

```python
from functools import partial

import jax
import jax.numpy as jnp
from jax import lax
from jax.experimental import pallas as pl
from jax.experimental.pallas import tpu as pltpu
from jax.sharding import PartitionSpec as P


D = 4096


RMS_EPS = 1e-06
GROUP_EPS = 0.00064


def swapped(shard, axis, stride):
    return lax.ppermute(shard, axis, [(i, i ^ 1 << stride) for i in range(lax.axis_size(axis))])


def for_sending(shard):

    def short(part):
        return part.astype(jnp.bfloat16) if part.dtype == jnp.float32 else part

    return jax.tree.map(short, shard)


def recurrent_update(
    layer_state,
    receptance_vector,
    key_vector,
    value_vector,
    decay_logits,
    learning_rate_logits,
    gate_logits,
    decay_constant,
    self_term_scale,
    head_gain_slice,
):
    highest = lax.Precision.HIGHEST
    shrink = jnp.exp(-jnp.exp(-jax.nn.softplus(-(decay_constant + decay_logits)) - 0.5))
    rate = jax.nn.sigmoid(learning_rate_logits)
    normed = key_vector * lax.rsqrt(jnp.sum(key_vector * key_vector, -1, keepdims=True) + 1.0)
    removed = jnp.einsum("...ij,...j->...i", layer_state, normed, precision=highest)
    layer_state = (
        layer_state * shrink[..., None, :]
        - removed[..., :, None] * (normed * rate)[..., None, :]
        + value_vector[..., :, None] * (key_vector * rate)[..., None, :]
    )
    readout = jnp.einsum("...ij,...j->...i", layer_state, receptance_vector, precision=highest)
    center = jnp.mean(readout, -1, keepdims=True)
    spread = jnp.mean(jnp.square(readout - center), -1, keepdims=True)
    normed_output = (readout - center) * lax.rsqrt(spread + GROUP_EPS) * head_gain_slice
    self_term = (
        jnp.sum(receptance_vector * key_vector * self_term_scale, -1, keepdims=True) * value_vector
    )
    return (
        ((normed_output + self_term) * jax.nn.sigmoid(gate_logits)).astype(jnp.bfloat16),
        layer_state,
    )


def double_gather(piece, position, first_bit, count, mover):
    for offset in range(count):
        which_bit = first_bit + offset
        partner = mover(piece, which_bit)
        lower_self = position >> which_bit & 1 == 0
        piece = jnp.where(
            lower_self, jnp.concatenate([piece, partner], 0), jnp.concatenate([partner, piece], 0)
        )
    return piece


def halve_sum(members, position, first_bit, count, mover):
    for offset in reversed(range(count)):
        which_bit = first_bit + offset
        upper_self = position >> which_bit & 1 == 1
        sends = tuple(
            (
                jnp.where(
                    upper_self, member[: member.shape[0] // 2], member[member.shape[0] // 2 :]
                )
                for member in members
            )
        )
        keeps = tuple(
            (
                jnp.where(
                    upper_self, member[member.shape[0] // 2 :], member[: member.shape[0] // 2]
                )
                for member in members
            )
        )
        arrived = mover(sends, which_bit)
        members = tuple((kept + got for kept, got in zip(keeps, arrived)))
    return members


def on_device_blocked(
    tokens,
    block_norm_gain,
    receptance_weight,
    key_weight,
    value_weight,
    decay_weight,
    learning_rate_weight,
    gate_weight,
    decay_bias_fixed,
    self_token_weight,
    readout_norm_gain,
    output_weight,
    state,
):
    columns_dev = tokens.shape[2]
    row_blocks = D // columns_dev
    low_bits = row_blocks.bit_length() - 1
    head_count = lax.axis_size("tp") // row_blocks
    high_bits = head_count.bit_length() - 1
    position = lax.axis_index("tp")
    head_index = position // row_blocks
    row_block = position % row_blocks
    head_size = receptance_weight.shape[3]
    seq_tile = tokens.shape[1]
    move_rows = lambda payload, which_bit: swapped(payload, "tp", which_bit)
    move_proj = lambda payload, which_bit: swapped(payload, "tp", which_bit)
    move_outs = lambda payload, which_bit: jax.tree.map(
        lambda part, own: part.astype(own.dtype),
        swapped(for_sending(payload), "tp", which_bit),
        payload,
    )
    move_split = lambda payload, which_bit: jax.tree.map(
        lambda part, own: part.astype(own.dtype),
        swapped(for_sending(payload), "tp", which_bit),
        payload,
    )

    def mixer(columns, layer_index):
        gain_cols = lax.dynamic_slice_in_dim(
            block_norm_gain[layer_index], row_block * columns_dev, columns_dev
        )
        wide = columns.astype(jnp.float32)
        scaled = (wide * gain_cols).astype(jnp.bfloat16)
        squares = jnp.sum(wide * wide, axis=1)
        weights = jnp.concatenate(
            [
                receptance_weight[layer_index, 0],
                key_weight[layer_index, 0],
                value_weight[layer_index, 0],
                decay_weight[layer_index, 0],
                learning_rate_weight[layer_index, 0],
                gate_weight[layer_index, 0],
            ],
            axis=1,
        )
        partial_value = jnp.dot(scaled, weights, preferred_element_type=jnp.float32)
        summed, total_sq = halve_sum((partial_value, squares), position, 0, low_bits, move_proj)
        projected = summed * lax.rsqrt(total_sq / D + RMS_EPS)[:, None]
        output_pieces = jnp.split(projected, 6, axis=1)

        def head_columns(table):
            return lax.dynamic_slice_in_dim(table[layer_index], head_index * head_size, head_size)

        layer_state = state[layer_index, 0].reshape(-1, head_size, head_size)
        out_tile, layer_state = recurrent_update(
            layer_state,
            *output_pieces,
            head_columns(decay_bias_fixed),
            head_columns(self_token_weight),
            head_columns(readout_norm_gain)
        )
        out_all = double_gather(out_tile, position, 0, low_bits, move_outs)
        branch = jnp.dot(out_all, output_weight[layer_index, 0], preferred_element_type=jnp.float32)
        return (branch, layer_state.reshape(layer_state.shape[0], head_size * head_size))

    columns = double_gather(tokens[0], position, low_bits, high_bits, move_rows)
    first_branch, first_memory = mixer(columns, 0)
    (tile_sum,) = halve_sum((first_branch,), position, low_bits, high_bits, move_split)
    tile_one = (tokens[0].astype(jnp.float32) + tile_sum).astype(jnp.bfloat16)
    columns = double_gather(tile_one, position, low_bits, high_bits, move_rows)
    second_branch, second_memory = mixer(columns, 1)
    (tile_sum,) = halve_sum((second_branch,), position, low_bits, high_bits, move_split)
    resid_rows = lax.dynamic_slice_in_dim(columns, head_index * seq_tile, seq_tile, 0)
    mixed = (resid_rows.astype(jnp.float32) + tile_sum).astype(jnp.bfloat16)
    new_state = jnp.stack([first_memory, second_memory])[:, None]
    return (mixed[None], new_state)


CORES = 2
PLANE = 4
STATE_ROWS = 64
FRONT_ROWS = 256


def moved(part, mask):
    return lax.ppermute(part, "tp", [(i, i ^ mask) for i in range(lax.axis_size("tp"))])


def near(part):
    return pltpu.with_memory_space_constraint(part, pltpu.VMEM)


def far(part):
    return pltpu.with_memory_space_constraint(part, pltpu.HBM)


def slots(place_ref, rows, seq_tile):
    chips = rows // seq_tile // CORES
    levels = chips // PLANE
    for off_core in range(CORES):
        for apart in range(PLANE):
            for level in range(levels):
                chip = place_ref[0] ^ (apart + PLANE * level)
                tile = chip * CORES + (place_ref[1] ^ off_core)
                yield pl.multiple_of(tile * seq_tile, seq_tile)


def load_kernel(place_ref, *refs, layer, layers, count, head_size, seq_tile):
    arrived, loaded = refs[-2:]
    refs = refs[:-2]
    split = (len(refs) + count - (layers if count else 0)) // 2
    (state_ref, *sources), (rows_ref, *targets) = refs[:split], refs[split:]
    pairs = [
        (ref.at[at_layer, 0], targets[at_layer].at[at * head_size : (at + 1) * head_size, :])
        for at_layer in range(layers if count else 0)
        for at, ref in enumerate(sources[:count])
    ] + list(zip(sources[count:], targets[layers:]))
    copies = [
        pltpu.make_async_copy(source, target, arrived.at[at])
        for at, (source, target) in enumerate(pairs)
    ]
    for copy in copies:
        copy.start()
    for slot, at in enumerate(slots(place_ref, rows_ref.shape[0], seq_tile)):
        pltpu.make_async_copy(
            state_ref.at[layer, 0, pl.ds(at, seq_tile)],
            rows_ref.at[slot * seq_tile : (slot + 1) * seq_tile],
            loaded,
        ).start()
    for copy in copies:
        copy.wait()
    pltpu.make_async_copy(state_ref.at[layer, 0], rows_ref, loaded).wait()


def load(place, state, layer, weights=(), tables=()):
    layers = state.shape[0]
    seqs = state.shape[2]
    outs = [pltpu.VMEM(state.shape[2:], state.dtype)]
    head_size = 0
    if weights:
        _, _, head_size, columns = weights[0].shape
        outs += [pltpu.VMEM((len(weights) * head_size, columns), jnp.bfloat16)] * layers
    outs += [pltpu.VMEM(table.shape, table.dtype) for table in tables]
    sources = [state, *weights, *tables]
    loaded = pl.pallas_call(
        partial(
            load_kernel,
            layer=layer,
            layers=layers,
            count=len(weights),
            head_size=head_size,
            seq_tile=seqs // lax.axis_size("tp"),
        ),
        in_specs=[pl.BlockSpec(memory_space=pltpu.SMEM)]
        + [pl.BlockSpec(memory_space=pltpu.HBM)] * len(sources),
        out_specs=[pl.BlockSpec(memory_space=pltpu.VMEM)] * len(outs),
        out_shape=outs,
        scratch_shapes=[
            pltpu.SemaphoreType.DMA((layers * len(weights) + len(tables) + 1,)),
            pltpu.SemaphoreType.DMA,
        ],
        compiler_params=pltpu.CompilerParams(vmem_limit_bytes=1 << 20),
    )(place, *[far(source) for source in sources])
    return tuple(loaded)


def front_kernel(place_ref, *refs, piece_rows, head_size, layer):
    pieces = refs[: len(piece_rows)]
    (
        gain_ref,
        bias_ref,
        self_ref,
        readout_ref,
        weights_ref,
        rows_ref,
        out_ref,
        vec_ref,
        scaled_ref,
        fold_ref,
    ) = refs[len(piece_rows) :]
    wide = 2 * head_size
    seqs, columns = rows_ref.shape
    core = place_ref[1]

    def own(ref):
        row = ref[layer : layer + 1, pl.ds(pl.multiple_of(place_ref[0] * wide, wide), wide)]
        return jnp.where(core == 0, row[:, :head_size], row[:, head_size:])

    gain = gain_ref[layer : layer + 1, :]
    sums = [None] * (seqs // 16)
    for ref, rows in zip(pieces, piece_rows):
        for at, row in enumerate(rows):
            part = ref[at * 16 : at * 16 + 16, :].astype(jnp.float32)
            scaled_ref[row : row + 16, :] = (part * gain).astype(jnp.bfloat16)
            sums[row // 16] = jnp.sum(part * part, axis=1, keepdims=True)
    projected = lax.dot_general(
        scaled_ref[...],
        weights_ref[...],
        (((1,), (1,)), ((), ())),
        preferred_element_type=jnp.float32,
    )
    at_row = lax.broadcasted_iota(jnp.int32, fold_ref.shape, 0) >> (head_size.bit_length() - 1)
    at_lane = lax.broadcasted_iota(jnp.int32, fold_ref.shape, 1)
    fold_ref[...] = jnp.where(at_row == at_lane, 1.0, 0.0).astype(jnp.bfloat16)
    total = jnp.concatenate(sums, 0)
    projected = projected * lax.rsqrt(total / scaled_ref.shape[1] + RMS_EPS)
    r, k, v, p, q, g = [projected[:, at * head_size : (at + 1) * head_size] for at in range(6)]
    decay = jnp.exp(jax.nn.sigmoid(own(bias_ref) + p) * (-(2.718281828459045**-0.5)))
    rate = jax.nn.sigmoid(q)
    kn = k * lax.rsqrt(jnp.sum(k * k, -1, keepdims=True) + 1.0)
    decay_r = decay * r
    twice = lambda part: jnp.concatenate([part, part], 1)
    kn_wide, decay_r_wide = twice(kn), twice(decay_r)
    repeats = columns // wide
    removed, kept = [], []
    for block in range(seqs // FRONT_ROWS):
        span = slice(block * FRONT_ROWS, (block + 1) * FRONT_ROWS)
        rows = rows_ref[span, :]
        by_kn = (rows * jnp.tile(kn_wide[span], (1, repeats))).astype(jnp.bfloat16)
        by_r = (rows * jnp.tile(decay_r_wide[span], (1, repeats))).astype(jnp.bfloat16)
        both = jnp.dot(
            jnp.concatenate([by_kn, by_r], 0), fold_ref[...], preferred_element_type=jnp.float32
        )
        removed.append(both[:FRONT_ROWS, :head_size])
        kept.append(both[FRONT_ROWS:, :head_size])
    removed, kept = jnp.concatenate(removed, 0), jnp.concatenate(kept, 0)
    kn_rate = kn * rate
    k_rate = k * rate
    row_sum = lambda part: jnp.sum(part, -1, keepdims=True)
    readout = kept - removed * row_sum(kn_rate * r) + v * row_sum(k_rate * r)
    center = jnp.mean(readout, -1, keepdims=True)
    spread = jnp.mean(jnp.square(readout - center), -1, keepdims=True)
    normed = (readout - center) * lax.rsqrt(spread + GROUP_EPS) * own(readout_ref)
    out = (normed + row_sum(r * k * own(self_ref)) * v) * jax.nn.sigmoid(g)
    out_ref[...] = out.astype(jnp.bfloat16)
    for at, pair in enumerate(
        (twice(decay), twice(kn_rate), twice(k_rate), jnp.concatenate([v, removed], 1))
    ):
        vec_ref[:, at * wide : (at + 1) * wide] = pair


def front(place, pieces, piece_rows, gain, tables, packed, rows, layer):
    seqs, columns = rows.shape
    head_size = packed.shape[0] // 6
    wide = 2 * head_size
    vmem = pl.BlockSpec(memory_space=pltpu.VMEM)
    return pl.pallas_call(
        partial(front_kernel, piece_rows=piece_rows, head_size=head_size, layer=layer),
        in_specs=[pl.BlockSpec(memory_space=pltpu.SMEM)]
        + [vmem] * (len(pieces) + 3 + len(tables)),
        out_specs=[vmem, vmem],
        scratch_shapes=[
            pltpu.VMEM((seqs, D), jnp.bfloat16),
            pltpu.VMEM((columns, wide), jnp.bfloat16),
        ],
        out_shape=[
            jax.ShapeDtypeStruct((seqs, head_size), jnp.bfloat16),
            jax.ShapeDtypeStruct((seqs, 4 * wide), jnp.float32),
        ],
        compiler_params=pltpu.CompilerParams(vmem_limit_bytes=36 << 20),
    )(place, *[near(piece) for piece in pieces], near(gain), *[near(t) for t in tables], near(packed), near(rows))


def update_kernel(place_ref, vec_ref, rows_ref, *refs, seq_tile, head_size, layer, part):
    out_ref, spread_ref, results_ref, written = refs[-4:]
    wide = 2 * head_size
    seqs, columns = rows_ref.shape
    repeats = columns // wide
    at_row = lax.broadcasted_iota(jnp.int32, spread_ref.shape, 0) & (head_size - 1)
    at_lane = lax.broadcasted_iota(jnp.int32, spread_ref.shape, 1) >> (head_size.bit_length() - 1)
    spread_ref[...] = jnp.where(at_row == at_lane, 1.0, 0.0).astype(jnp.bfloat16)
    tiles = list(slots(place_ref, seqs, seq_tile))
    per_block = STATE_ROWS // seq_tile
    blocks = seqs // STATE_ROWS // CORES
    blocks = range(part * blocks, (part + 1) * blocks)
    for block in blocks:
        span = slice(block * STATE_ROWS, (block + 1) * STATE_ROWS)
        local = slice(
            (block - blocks[0]) * STATE_ROWS, (block - blocks[0] + 1) * STATE_ROWS
        )
        pair = vec_ref[span, 3 * wide :]
        high = pair.astype(jnp.bfloat16)
        low = (pair - high.astype(jnp.float32)).astype(jnp.bfloat16)

        def spread(at):
            lanes = slice(at * head_size, (at + 1) * head_size)
            both = jnp.concatenate([high[:, lanes], low[:, lanes]], 1)
            return jnp.dot(both, spread_ref[...], preferred_element_type=jnp.float32)

        row = lambda at: jnp.tile(vec_ref[span, at * wide : (at + 1) * wide], (1, repeats))
        results_ref[local, :] = rows_ref[span, :] * row(0) - spread(1) * row(1) + spread(0) * row(2)
        for slot in range(block * per_block, (block + 1) * per_block):
            at = slot * seq_tile - blocks[0] * STATE_ROWS
            pltpu.make_async_copy(
                results_ref.at[at : at + seq_tile],
                out_ref.at[layer, 0, pl.ds(tiles[slot], seq_tile)],
                written.at[block - blocks[0]],
            ).start()
    for at in range(len(blocks)):
        span = slice(at * STATE_ROWS, (at + 1) * STATE_ROWS)
        pltpu.make_async_copy(
            results_ref.at[span], out_ref.at[layer, 0, :STATE_ROWS], written.at[at]
        ).wait()


def update(place, vec, rows, previous, shape, layer, part):
    seqs, columns = rows.shape
    head_size = vec.shape[1] // 8
    vmem = pl.BlockSpec(memory_space=pltpu.VMEM)
    hbm = pl.BlockSpec(memory_space=pltpu.HBM)
    more = [previous] if previous is not None else []
    return pl.pallas_call(
        partial(
            update_kernel,
            seq_tile=seqs // lax.axis_size("tp"),
            head_size=head_size,
            layer=layer,
            part=part,
        ),
        in_specs=[pl.BlockSpec(memory_space=pltpu.SMEM), vmem, vmem] + [hbm] * len(more),
        out_specs=hbm,
        scratch_shapes=[
            pltpu.VMEM((2 * head_size, columns), jnp.bfloat16),
            pltpu.VMEM((seqs // CORES, columns), jnp.float32),
            pltpu.SemaphoreType.DMA((seqs // STATE_ROWS // CORES,)),
        ],
        out_shape=jax.ShapeDtypeStruct(shape, rows.dtype),
        input_output_aliases={3: 0} if more else {},
        compiler_params=pltpu.CompilerParams(vmem_limit_bytes=24 << 20),
    )(place, near(vec), near(rows), *more)


def gather_tiles(tile, levels):
    step = CORES * PLANE
    corner = moved(tile, CORES * 3)
    column = {at: moved(tile, step * at) for at in range(1, levels)}
    corners = {at: moved(corner, step * at) for at in range(1, levels)}
    column = jnp.concatenate([tile, *column.values()], 0)
    across = [moved(column, CORES * q) for q in (1, 2)]
    corners = jnp.concatenate([corner, *corners.values()], 0)
    pieces = [column, *across, corners]
    pieces += [moved(piece, 1) for piece in pieces]
    block = column.shape[0]
    places = [[at * block + r for r in range(0, block, 16)] for at in range(len(pieces))]
    return pieces, places


def sum_tiles(parts, levels, new_state, update_part):
    rows = parts.shape[0] // (PLANE * levels)
    block = levels * rows
    step = CORES * PLANE
    wide = lambda got: [part.astype(jnp.float32) for part in got]
    across = [moved(parts[q * block : (q + 1) * block], CORES * q) for q in (1, 2)]
    diagonal = parts[3 * block :]
    along = [moved(diagonal[at * rows : (at + 1) * rows], step * at) for at in range(1, levels)]
    new_state = update_part(new_state, 0)
    *across, new_state = lax.optimization_barrier((*across, new_state))
    summed = sum(wide([parts[:block], *across]))
    sends = summed.astype(jnp.bfloat16)
    got = [moved(sends[at * rows : (at + 1) * rows], step * at) for at in range(1, levels)]
    corner = sum(wide([diagonal[:rows], *along])).astype(jnp.bfloat16)
    got.append(moved(corner, CORES * 3))
    new_state = update_part(new_state, 1)
    *got, new_state = lax.optimization_barrier((*got, new_state))
    return summed[:rows] + sum(wide(got)), new_state


def on_device_whole(
    tokens,
    block_norm_gain,
    receptance_weight,
    key_weight,
    value_weight,
    decay_weight,
    learning_rate_weight,
    gate_weight,
    decay_bias_fixed,
    self_token_weight,
    readout_norm_gain,
    output_weight,
    state,
):
    devices = lax.axis_size("tp")
    levels = devices // (CORES * PLANE)
    position = lax.axis_index("tp")
    place = jnp.stack([position // CORES, position % CORES]).astype(jnp.int32)
    weights = [
        jnp.swapaxes(w, 2, 3)
        for w in (
            receptance_weight,
            key_weight,
            value_weight,
            decay_weight,
            learning_rate_weight,
            gate_weight,
        )
    ]
    tables = (decay_bias_fixed, self_token_weight, readout_norm_gain)
    own_out = output_weight[:, 0]
    other_out = moved(own_out, 1)

    tile, place = lax.optimization_barrier((tokens[0], place))
    new_state = None
    layers = state.shape[0]
    for layer in range(layers):
        pieces, places = gather_tiles(tile, levels)
        if layer == 0:
            loaded = load(place, state, layer, weights, (block_norm_gain, *tables))
            packed, (gain, *tables) = loaded[1 : 1 + layers], loaded[1 + layers :]
        else:
            loaded = load(place, state, layer)
        rows = loaded[0]
        out, vec = front(place, pieces, places, gain, tables, packed[layer], rows, layer)
        half = out.shape[0] // CORES
        parts = jnp.dot(out[:half], own_out[layer], preferred_element_type=jnp.float32)
        swapped = moved(out[half:], 1)
        parts = lax.optimization_barrier(parts)
        parts += jnp.dot(swapped, other_out[layer], preferred_element_type=jnp.float32)
        parts = parts.astype(jnp.bfloat16)
        parts, vec = lax.optimization_barrier((parts, vec))
        update_part = lambda previous, part: update(
            place, vec, rows, previous, state.shape, layer, part
        )
        total, new_state = sum_tiles(parts, levels, new_state, update_part)
        tile = (tile.astype(jnp.float32) + total).astype(jnp.bfloat16)
    return (tile[None], new_state)


def on_device(tokens, *rest):
    if tokens.shape[2] == D and lax.axis_size("tp") >= 16:
        return on_device_whole(tokens, *rest)
    return on_device_blocked(tokens, *rest)


def solution(mesh):
    return jax.shard_map(
        on_device,
        mesh=mesh,
        in_specs=(
            P("tp", None, None),
            P(),
            P(None, "tp", None, None),
            P(None, "tp", None, None),
            P(None, "tp", None, None),
            P(None, "tp", None, None),
            P(None, "tp", None, None),
            P(None, "tp", None, None),
            P(),
            P(),
            P(),
            P(None, "tp", None, None),
            P(None, "tp", None, None),
        ),
        out_specs=(P("tp", None, None), P(None, "tp", None, None)),
        check_vma=False,
    )
```
